768 devices in a mesh: fs: 24 (over z, core), tp: 32 (over y, x).
Axes of the slice: x: 4, y: 8, z: 12, core: 2. Of those that a mesh axis runs over, the one named last changes fastest.
Arguments:
- grad_gate: float32 [2112, 5632], P('fs', 'tp'), may hold values from -45 to 45
- grad_up: float32 [2112, 5632], P('fs', 'tp'), may hold values from -45 to 45
- moment_gate: float32 [2112, 5632], P('fs', 'tp'), may hold values from -6 to 6
- moment_up: float32 [2112, 5632], P('fs', 'tp'), may hold values from -6 to 6
Outputs:
- moment_gate_next: float32 [2112, 5632], P('fs', 'tp')
- moment_up_next: float32 [2112, 5632], P('fs', 'tp')
- update_gate: float32 [2112, 5632], P('fs', 'tp')
- update_up: float32 [2112, 5632], P('fs', 'tp')
The draws below stay inside these ranges and needn't reach their ends.
All inputs are finite; a program needn't handle non-finite values.
Results may differ from the reference program's by a relative error of at most 0.0019.
The reference program's roundings to bfloat16 on the way (of `poly_low` and `product_low`) count: a program that leaves them out, or rounds other values in their place, can miss the bound.
Values may be sent and summed in bfloat16 or wider, within the bound.
No kernel may reach another device: no remote copies, remote signals or barrier semaphores. Data moves between devices by JAX's collectives and lax.ppermute only.
A program may use at most 32 MiB of HBM per device.

```python
import math
import jax
import jax.numpy as jnp

D = 2112
FF = 5632
ITERS = 3


def scaled_noise(key):
    key_rows, key_cols, key_base = jax.random.split(key, 3)
    row_scales = jnp.exp(jax.random.uniform(key_rows, (D, 1), jnp.float32, 0.0, math.log(10.0)))
    col_scales = jnp.exp(jax.random.uniform(key_cols, (1, FF), jnp.float32, 0.0, math.log(3.0)))
    base = jnp.clip(jax.random.normal(key_base, (D, FF), jnp.float32), -6.0, 6.0)
    return base * row_scales * col_scales / 4.0


def draw_grad_gate(key, part):
    return scaled_noise(jax.random.fold_in(key, 11))


def draw_grad_up(key, part):
    return scaled_noise(jax.random.fold_in(key, 23))


def block_levels(key, shape, pieces, least, high):
    factor_of = 1.0
    for axis_at, parts in pieces:
        steps = jax.random.uniform(jax.random.fold_in(jax.random.fold_in(key, 6), axis_at), (parts,), jnp.float32, least / len(pieces), high / len(pieces))
        factor_of = factor_of * jnp.repeat(jnp.exp(steps), shape[axis_at] // parts).reshape((-1,) + (1,) * (len(shape) - 1 - axis_at))
    return factor_of


def normal_values(own_key, shape, width, bound, cuts=(), held_as=jnp.bfloat16):
    drawn = width * jax.random.normal(own_key, shape, jnp.float32)
    if cuts:
        drawn = drawn * block_levels(own_key, shape, cuts, -0.22, 0.18)
    return jnp.clip(drawn, -bound, bound).astype(held_as)


def setup_inputs(seed: int = 0) -> dict:
    arg_keys = jax.random.split(jax.random.key(seed), 5)
    grad_gate = draw_grad_gate(jax.random.fold_in(arg_keys[4], 71), 0)
    grad_up = draw_grad_up(jax.random.fold_in(arg_keys[4], 71), 0)
    moment_gate = normal_values(arg_keys[2], (D, FF), 1.0, 6.0, ((0, 24), (1, 32)), jnp.float32)
    moment_up = normal_values(arg_keys[3], (D, FF), 1.0, 6.0, ((0, 24), (1, 32)), jnp.float32)
    return {"grad_gate": grad_gate, "grad_up": grad_up, "moment_gate": moment_gate, "moment_up": moment_up}


BETA = 0.95
EPS = 1e-06

def reference(grad_gate, grad_up, moment_gate, moment_up):
    moment_gate_next = BETA * moment_gate + grad_gate
    moment_up_next = BETA * moment_up + grad_up
    low_gate = moment_gate_next.astype(jnp.bfloat16)
    low_up = moment_up_next.astype(jnp.bfloat16)
    gram = jnp.dot(low_gate, low_gate.T, preferred_element_type=jnp.float32) + jnp.dot(low_up, low_up.T, preferred_element_type=jnp.float32)
    trace_total = jnp.sum(jnp.square(low_gate.astype(jnp.float32))) + jnp.sum(jnp.square(low_up.astype(jnp.float32)))
    square_total = jnp.sum(gram * gram)
    spectral = 2.0 * square_total / (trace_total + EPS)
    current = gram / spectral
    identity = jnp.eye(D, dtype=jnp.float32)
    product_low = None
    for iteration in range(ITERS):
        poly_low = (1.5 * identity - 0.5 * current).astype(jnp.bfloat16)
        if iteration == 0:
            product_low = poly_low
        else:
            product_low = jnp.dot(product_low, poly_low, preferred_element_type=jnp.float32).astype(jnp.bfloat16)
        if iteration < ITERS - 1:
            square_low = jnp.dot(poly_low, poly_low, preferred_element_type=jnp.float32).astype(jnp.bfloat16)
            current = jnp.dot(current.astype(jnp.bfloat16), square_low, preferred_element_type=jnp.float32)
    factor = jnp.sqrt(2.0 * FF / spectral)
    update_gate = jnp.dot(product_low.T, low_gate, preferred_element_type=jnp.float32) * factor
    update_up = jnp.dot(product_low.T, low_up, preferred_element_type=jnp.float32) * factor
    return (moment_gate_next, moment_up_next, update_gate, update_up)
```

```python
import jax
import jax.numpy as jnp
from jax import lax
from jax.sharding import Mesh
from jax.sharding import PartitionSpec as P

FF = 5632
FS = ("z", "core")
TP = ("y", "x")
BETA = 0.95
EPS = 1e-06


def dot(left, right):
    return jnp.dot(left, right, preferred_element_type=jnp.float32)


def to_all(block, axes):
    copies = jnp.broadcast_to(block, (lax.axis_size(axes), *block.shape))
    return lax.all_to_all(copies, axes, split_axis=0, concat_axis=0, tiled=True)


def rows_of(blocks):
    return jnp.moveaxis(blocks, 0, 1).reshape(blocks.shape[1], -1)


def gather_rows(block):
    by_z = lax.all_gather(block, "z")
    both = lax.all_gather(by_z, "core")
    return jnp.swapaxes(both, 0, 1).reshape(-1, *block.shape)


def local(grad_gate, grad_up, moment_gate, moment_up):
    gate_next = BETA * moment_gate + grad_gate
    up_next = BETA * moment_up + grad_up
    low = jnp.concatenate([gate_next.astype(jnp.bfloat16), up_next.astype(jnp.bfloat16)], axis=1)
    rows_dev, half = gate_next.shape
    by_z = lax.all_gather(low, "z")
    gate_all = gather_core(by_z[..., :half])
    up_all = gather_core(by_z[..., half:])
    width = gate_all.shape[0]
    own_rows = width // lax.axis_size(TP)
    share = lax.dot_general(
        gate_all, low[:, :half], (((1,), (1,)), ((), ())), preferred_element_type=jnp.float32
    ) + lax.dot_general(
        up_all, low[:, half:], (((1,), (1,)), ((), ())), preferred_element_type=jnp.float32
    )
    blocks = share.reshape(-1, own_rows, rows_dev)
    arrived = lax.all_to_all(blocks, TP, split_axis=0, concat_axis=0, tiled=True)
    gram = arrived.sum(axis=0)

    rows_at = lax.axis_index(TP) * own_rows
    cols_at = lax.axis_index(FS) * rows_dev

    def eye_of(shape, row, col):
        i = row + lax.broadcasted_iota(jnp.int32, shape, 0)
        j = col + lax.broadcasted_iota(jnp.int32, shape, 1)
        return i == j

    own_eye = eye_of((own_rows, rows_dev), rows_at, cols_at)
    rows_eye = eye_of((own_rows, width), rows_at, 0)
    cols_eye = eye_of((width, rows_dev), 0, cols_at)

    gram_rows = rows_of(gather_rows(gram))
    square = jnp.sum(gram_rows * gram_rows)
    trace = jnp.sum(jnp.where(rows_eye, gram_rows, 0.0))
    tail = jnp.zeros((own_rows, 2), jnp.float32) + jnp.stack([square, trace])[None, :]
    sent = jnp.concatenate([gram, tail], axis=1)
    arrived = to_all(sent, TP)
    gram_cols = arrived[..., :rows_dev].reshape(width, rows_dev)
    totals = arrived[:, 0, rows_dev:].sum(axis=0)
    spectral = 2.0 * totals[0] / (totals[1] + EPS)

    def poly(eye, current):
        return jnp.where(eye, 1.5 - 0.5 * current, -0.5 * current).astype(jnp.bfloat16)

    current_rows = gram_rows / spectral
    poly_rows = poly(rows_eye, current_rows)
    current_rows = current_rows.astype(jnp.bfloat16)
    poly_cols = poly(cols_eye, gram_cols / spectral)

    square_low = dot(poly_rows, poly_cols).astype(jnp.bfloat16)
    square_cols = to_all(square_low, TP).reshape(width, rows_dev)
    current = dot(current_rows, square_cols)
    poly_low = poly(own_eye, current)
    diag = jnp.sum(jnp.where(own_eye, current, 0.0), axis=1, keepdims=True).astype(jnp.bfloat16)

    poly_cols = to_all(poly_low, TP).reshape(width, rows_dev)
    blocks = gather_rows(jnp.concatenate([poly_low, diag], axis=1))
    first_rows = rows_of(blocks[..., :rows_dev])
    diag = blocks[..., rows_dev].astype(jnp.float32).sum(axis=0)
    current_rows = jnp.where(
        rows_eye, diag[:, None], -2.0 * first_rows.astype(jnp.float32)
    ).astype(jnp.bfloat16)

    product_low = dot(poly_rows, poly_cols).astype(jnp.bfloat16)
    square_low = dot(first_rows, poly_cols).astype(jnp.bfloat16)
    square_cols = to_all(square_low, TP).reshape(width, rows_dev)
    product_rows = rows_of(gather_rows(product_low))
    current = dot(current_rows, square_cols)
    poly_low = poly(own_eye, current)
    poly_cols = to_all(poly_low, TP).reshape(width, rows_dev)
    product_low = dot(product_rows, poly_cols).astype(jnp.bfloat16)
    product_cols = to_all(product_low, TP).reshape(width, rows_dev)

    factor = jnp.sqrt(2.0 * FF / spectral)
    over_rows = (((0,), (0,)), ((), ()))
    ortho_gate = lax.dot_general(product_cols, gate_all, over_rows, preferred_element_type=jnp.float32)
    ortho_up = lax.dot_general(product_cols, up_all, over_rows, preferred_element_type=jnp.float32)
    return gate_next, up_next, ortho_gate * factor, ortho_up * factor


def gather_core(by_z):
    both = lax.all_gather(by_z, "core")
    return jnp.swapaxes(both, 0, 1).reshape(-1, by_z.shape[-1])


def solution(mesh):
    split = Mesh(mesh.devices.reshape(12, 2, 8, 4), ("z", "core", "y", "x"))
    spec = P(FS, TP)
    return jax.shard_map(
        local, mesh=split, in_specs=(spec,) * 4, out_specs=(spec,) * 4, check_vma=False
    )
```

```python
import functools

import jax
import jax.numpy as jnp
from jax import lax
from jax.experimental import pallas as pl
from jax.experimental.pallas import tpu as pltpu
from jax.sharding import Mesh
from jax.sharding import PartitionSpec as P

FF = 5632
FS = ("z", "core")
TP = ("y", "x")
BETA = 0.95
EPS = 1e-06
D = 2112
COLS = 88
ROWS = 72
LANES = 128
DEPTH = 12
NEAR = 6
TPS = 32
PACK = 56
SPARE = 48
KDIM = (D // COLS) * LANES
f32, bf16 = jnp.float32, jnp.bfloat16


def place(core, z):
    return ((z // NEAR) * 2 + core) * NEAR + z % NEAR


def lanes_of(rows):
    return lax.broadcasted_iota(jnp.int32, (rows, LANES), 1)


def rows_of(rows):
    return lax.broadcasted_iota(jnp.int32, (rows, LANES), 0)


def pack(block, tail=None):
    lane = lanes_of(16)
    low = block[PACK:ROWS]
    parts = [
        jnp.where(lane < COLS, block[16 * i : 16 * i + 16], pltpu.roll(low, shift, 1))
        for i, shift in enumerate((COLS, COLS - 40, COLS - 80))
    ]
    end = block[SPARE:PACK]
    if tail is not None:
        end = jnp.where(lanes_of(PACK - SPARE) < COLS, end, tail)
    return jnp.concatenate([*parts, end], axis=0)


def low_rows(packed):
    lane = lanes_of(16)
    a, b, c = (
        pltpu.roll(packed[16 * i : 16 * i + 16].astype(f32), shift, 1)
        for i, shift in enumerate((40, 80, 120))
    )
    return jnp.where(lane < 40, a, jnp.where(lane < 80, b, c))


def store_rows(target, first, value):
    at, last = first, min(first + value.shape[0], D)
    while at < last:
        block, row = divmod(at, COLS)
        count = min(COLS - row, last - at)
        start = block * LANES + row
        target[start : start + count, :] = value[at - first : at - first + count].astype(target.dtype)
        at += count


def clear_gaps(target):
    for block in range(D // COLS):
        target[block * LANES + COLS : (block + 1) * LANES, :] = jnp.zeros((LANES - COLS, LANES), target.dtype)


def unpack_columns(blocks, target, change=None):
    clear_gaps(target)
    for t in range(-(-D // ROWS)):
        packed = blocks[t]
        for first, part in ((ROWS * t, packed), (ROWS * t + PACK, low_rows(packed))):
            store_rows(target, first, change(part, first) if change else part)


def unpack_rows(blocks, targets, change):
    for core in range(2):
        for z in range(DEPTH):
            b = place(core, z)
            packed = blocks[core, z]
            for first, part in ((0, packed), (PACK, low_rows(packed))):
                for target, value in zip(targets, change(part, first, b * COLS, packed)):
                    target[first : first + part.shape[0], b * LANES : (b + 1) * LANES] = value


def poly(eye, current):
    return jnp.where(eye, 1.5 - 0.5 * current, -0.5 * current)


def dot(left, right):
    return jnp.dot(left, right, preferred_element_type=f32)


def copies(out, value):
    for i in range(out.shape[0]):
        out[i] = value


def gram_kernel(low, whole0, whole1, out, own, share):
    own[:COLS] = low[...]
    own[COLS:] = jnp.zeros((LANES - COLS, own.shape[1]), bf16)
    half = D // 2
    for h, whole in enumerate((whole0, whole1)):
        share[h * half : (h + 1) * half] = lax.dot_general(
            whole[...], own[...], (((1,), (1,)), ((), ())), preferred_element_type=f32
        )
    share[D:] = jnp.zeros((share.shape[0] - D, LANES), f32)
    filled = -(-D // ROWS)
    for t in range(filled):
        out[t] = pack(share[ROWS * t : ROWS * (t + 1)])
    for t in range(filled, TPS):
        out[t] = jnp.zeros((PACK, LANES), f32)


def total_kernel(trace, arrived, gram, out):
    total = arrived[0]
    for t in range(1, TPS):
        total += arrived[t]
    gram[...] = total
    tail = jnp.where(lanes_of(PACK) == COLS, trace[0, 0], total)
    spot = (rows_of(PACK) == SPARE) & (lanes_of(PACK) == COLS)
    copies(out, jnp.where(spot, tail, total))


def square_kernel(gram, rows, out):
    square = jnp.zeros((PACK, LANES), f32)
    trace = jnp.zeros((PACK, LANES), f32)
    free = (rows_of(PACK) >= SPARE) & (lanes_of(PACK) >= COLS)
    for core in range(2):
        for z in range(DEPTH):
            value = rows[core, z]
            square += value * value
            trace += value
    square = jnp.sum(jnp.where(free, 0.0, square), keepdims=True)
    trace = jnp.sum(jnp.where(free, trace, 0.0), keepdims=True)
    spot = rows_of(PACK) == SPARE
    value = jnp.where(spot & (lanes_of(PACK) == COLS), square, gram[...])
    copies(out, jnp.where(spot & (lanes_of(PACK) == COLS + 1), trace, value))


def first_kernel(at, rows, cols, out, poly_rows, current_rows, spectral_out, right):
    row0, col0 = at[0], at[1]
    tails = cols[0, SPARE:PACK]
    for t in range(1, TPS):
        tails += cols[t, SPARE:PACK]
    spot = rows_of(PACK - SPARE) == 0
    lane = lanes_of(PACK - SPARE)
    square = jnp.sum(jnp.where(spot & (lane == COLS), tails, 0.0), keepdims=True)
    trace = jnp.sum(jnp.where(spot & (lane == COLS + 1), tails, 0.0), keepdims=True)
    spectral = 2.0 * square / (trace + EPS)
    inverse = 1.0 / spectral
    spectral_out[...] = jnp.broadcast_to(spectral, spectral_out.shape)

    def of_cols(part, first):
        n = part.shape[0]
        eye = rows_of(n) + first == lanes_of(n) + col0
        return poly(eye, part * inverse)

    unpack_columns(cols, right, of_cols)

    def of_rows(part, first, col, packed):
        n = part.shape[0]
        eye = (rows_of(n) + (row0 + first) == lanes_of(n) + col) & (lanes_of(n) < COLS)
        current = part * inverse
        return poly(eye, current).astype(bf16), current.astype(bf16)

    unpack_rows(rows, (poly_rows, current_rows), of_rows)
    copies(out, pack(dot(poly_rows[...], right[...])).astype(bf16))


def next_poly(at, left, right):
    current = dot(left, right)
    eye = (rows_of(ROWS) + at[0] == lanes_of(ROWS) + at[1]) & (lanes_of(ROWS) < COLS)
    return poly(eye, current), jnp.sum(jnp.where(eye, current, 0.0), axis=0, keepdims=True)


def second_kernel(at, current_rows, cols, out_cols, out_rows, right):
    unpack_columns(cols, right)
    value, diag = next_poly(at, current_rows[...], right[...])
    diag = jnp.broadcast_to(diag, (PACK - SPARE, LANES))
    row = rows_of(PACK - SPARE)
    tail = jnp.where(
        row == 0,
        pltpu.roll(diag, COLS, 1),
        jnp.where(row == 1, pltpu.roll(diag, COLS - 40, 1), pltpu.roll(diag, COLS - 80, 1)),
    )
    value = pack(value, tail).astype(bf16)
    copies(out_cols, value)
    copies(out_rows, value)


def third_kernel(at, poly_rows, rows, cols, out_square, out_product, current_rows, first_rows, right):
    row0 = at[0]
    unpack_columns(cols, right)
    copies(out_product, pack(dot(poly_rows[...], right[...])).astype(bf16))

    def of_rows(part, first, col, packed):
        n = part.shape[0]
        eye = (rows_of(n) + (row0 + first) == lanes_of(n) + col) & (lanes_of(n) < COLS)
        tail = packed[SPARE:PACK].astype(f32)
        lane = lanes_of(1)
        diag = jnp.where(
            lane < 40,
            pltpu.roll(tail, 40, 1)[0:1],
            jnp.where(lane < 80, pltpu.roll(tail, 80, 1)[1:2], pltpu.roll(tail, 120, 1)[2:3]),
        )
        part = part.astype(f32)
        return part.astype(bf16), jnp.where(eye, diag, -2.0 * part).astype(bf16)

    unpack_rows(rows, (first_rows, current_rows), of_rows)
    copies(out_square, pack(dot(first_rows[...], right[...])).astype(bf16))


def fourth_kernel(at, current_rows, cols, out, right):
    unpack_columns(cols, right)
    copies(out, pack(next_poly(at, current_rows[...], right[...])[0]).astype(bf16))


def fifth_kernel(rows, cols, out, product_rows, right):
    unpack_columns(cols, right)
    unpack_rows(rows, (product_rows,), lambda part, first, col, packed: (part.astype(bf16),))
    copies(out, pack(dot(product_rows[...], right[...])).astype(bf16))


def last_kernel(cols, out):
    for t in range(-(-D // ROWS)):
        packed = cols[t]
        count = min(ROWS, D - ROWS * t)
        top = min(count, PACK)
        out[ROWS * t : ROWS * t + top, :] = packed[:top]
        if count > PACK:
            out[ROWS * t + PACK : ROWS * (t + 1), :] = low_rows(packed).astype(bf16)


def call(kernel, outs, *args, scratch=(), flops=0):
    vmem = pl.BlockSpec(memory_space=pltpu.VMEM)
    smem = pl.BlockSpec(memory_space=pltpu.SMEM)
    return pl.pallas_call(
        kernel,
        out_shape=[jax.ShapeDtypeStruct(shape, dtype) for shape, dtype in outs],
        in_specs=[smem if a.size < 8 else vmem for a in args],
        out_specs=[vmem] * len(outs),
        scratch_shapes=[pltpu.VMEM(shape, dtype) for shape, dtype in scratch],
        compiler_params=pltpu.CompilerParams(vmem_limit_bytes=24 * 2**20),
        name=kernel.__name__,
    )(*args)


def exchange(stacked, axes):
    return lax.all_to_all(stacked, axes, split_axis=0, concat_axis=0, tiled=True)


def both_cores(by_z):
    return lax.all_gather(by_z, "core")


def local(grad_gate, grad_up, moment_gate, moment_up):
    gate_next = BETA * moment_gate + grad_gate
    up_next = BETA * moment_up + grad_up
    half = gate_next.shape[1]
    low = jnp.concatenate([gate_next.astype(bf16), up_next.astype(bf16)], axis=1)
    low = jnp.pad(low, ((0, 0), (0, 3 * LANES - 2 * half)))
    trace = jnp.sum(jnp.square(low.astype(f32))).reshape(1, 1)
    by_z = lax.all_gather(low, "z")
    whole = [
        lax.all_gather(by_z[h * NEAR : (h + 1) * NEAR], "core").reshape(D // 2, -1) for h in range(2)
    ]
    z, core, t = lax.axis_index("z"), lax.axis_index("core"), lax.axis_index(TP)
    at = jnp.stack([t * ROWS, place(core, z) * COLS]).astype(jnp.int32)

    right = ((KDIM, LANES), bf16)
    left = ((ROWS, KDIM), bf16)
    to_tp, to_z = ((TPS, PACK, LANES), bf16), ((DEPTH, PACK, LANES), bf16)
    to_tp32, to_z32 = ((TPS, PACK, LANES), f32), ((DEPTH, PACK, LANES), f32)

    (shares,) = call(
        gram_kernel,
        [to_tp32],
        low,
        *whole,
        scratch=[((LANES, low.shape[1]), bf16), ((-(-D // ROWS) * ROWS, LANES), f32)],
    )
    gram, sent = call(total_kernel, [((PACK, LANES), f32), to_z32], trace, exchange(shares, TP))
    gram_rows = both_cores(exchange(sent, "z"))
    (sent,) = call(square_kernel, [to_tp32], gram, gram_rows)
    sent, poly_rows, current_rows, spectral = call(
        first_kernel,
        [to_tp, left, left, ((8, LANES), f32)],
        at,
        gram_rows,
        exchange(sent, TP),
        scratch=[right],
    )
    cols, rows = call(second_kernel, [to_tp, to_z], at, current_rows, exchange(sent, TP), scratch=[right])
    square, product, current_rows = call(
        third_kernel,
        [to_tp, to_z, left],
        at,
        poly_rows,
        both_cores(exchange(rows, "z")),
        exchange(cols, TP),
        scratch=[left, right],
    )
    (cols,) = call(fourth_kernel, [to_tp], at, current_rows, exchange(square, TP), scratch=[right])
    (cols,) = call(
        fifth_kernel,
        [to_tp],
        both_cores(exchange(product, "z")),
        exchange(cols, TP),
        scratch=[left, right],
    )
    (product,) = call(last_kernel, [((D, LANES), bf16)], exchange(cols, TP))
    over_rows = (((0,), (0,)), ((), ()))
    ortho = sum(
        lax.dot_general(
            product[h * D // 2 : (h + 1) * D // 2, :COLS], whole[h], over_rows, preferred_element_type=f32
        )
        for h in range(2)
    )
    ortho = ortho * jnp.sqrt(2.0 * FF / spectral[0, 0])
    return gate_next, up_next, ortho[:, :half], ortho[:, half : 2 * half]


def solution(mesh):
    split = Mesh(mesh.devices.reshape(DEPTH, 2, 8, 4), ("z", "core", "y", "x"))
    spec = P(FS, TP)
    return jax.shard_map(
        local, mesh=split, in_specs=(spec,) * 4, out_specs=(spec,) * 4, check_vma=False
    )
```

```python
import jax
import jax.numpy as jnp
from jax import lax
from jax.experimental import pallas as pl
from jax.experimental.pallas import tpu as pltpu
from jax.sharding import Mesh
from jax.sharding import PartitionSpec as P

FF = 5632
FS = ("z", "core")
TP = ("y", "x")
BETA = 0.95
EPS = 1e-06
LANES = 128
D = 2112
COLS = 88
BLOCKS = D // COLS
DEPTH = 12
NEAR = 6
TPS = 32
MAIN = 64
SHARED = TPS * MAIN
ROWS = MAIN + 8
PIECE = COLS // 4
SENT = 48
WIDE = 56
FREE = 96
SPARE = 48
KDIM = BLOCKS * LANES
f32, bf16 = jnp.float32, jnp.bfloat16


def place(core, z):
    return ((z // NEAR) * 2 + core) * NEAR + z % NEAR


def lanes_of(rows):
    return lax.broadcasted_iota(jnp.int32, (rows, LANES), 1)


def rows_of(rows):
    return lax.broadcasted_iota(jnp.int32, (rows, LANES), 0)


def folded(block, low):
    lane = lanes_of(16)
    return [
        jnp.where(lane < COLS, block[16 * i : 16 * i + 16], pltpu.roll(low, shift, 1))
        for i, shift in enumerate((COLS, COLS - 40, COLS - 80))
    ]


def unfolded(packed):
    lane = lanes_of(16)
    a, b, c = (
        pltpu.roll(packed[16 * i : 16 * i + 16].astype(f32), shift, 1)
        for i, shift in enumerate((40, 80, 120))
    )
    return jnp.where(lane < 40, a, jnp.where(lane < 80, b, c))


def pack_tp(main, shared, shift, tail=None):
    a, b, c = folded(main, main[48:64])
    top = jnp.where(lanes_of(8) < FREE, c[:8], pltpu.roll(shared, shift, 1))
    end = c[8:] if tail is None else jnp.where(lanes_of(8) < FREE, c[8:], tail)
    return jnp.concatenate([a, b, top, end], axis=0)


def pack_z(block, tail=None):
    end = block[SPARE:WIDE]
    if tail is not None:
        end = jnp.where(lanes_of(WIDE - SPARE) < COLS, end, tail)
    return jnp.concatenate([*folded(block, block[WIDE:ROWS]), end], axis=0)


def spread(row):
    row = jnp.broadcast_to(row, (WIDE - SPARE, LANES))
    at = rows_of(WIDE - SPARE)
    return jnp.where(
        at == 0,
        pltpu.roll(row, COLS, 1),
        jnp.where(at == 1, pltpu.roll(row, COLS - 40, 1), pltpu.roll(row, COLS - 80, 1)),
    )


def gathered(packed):
    tail = packed[SPARE:WIDE].astype(f32)
    lane = lanes_of(1)
    return jnp.where(
        lane < 40,
        pltpu.roll(tail, 40, 1)[0:1],
        jnp.where(lane < 80, pltpu.roll(tail, 80, 1)[1:2], pltpu.roll(tail, 120, 1)[2:3]),
    )


def store_rows(target, first, value):
    at, last = first, first + value.shape[0]
    while at < last:
        block, row = divmod(at, COLS)
        count = min(COLS - row, last - at)
        start = block * LANES + row
        target[start : start + count, :] = value[at - first : at - first + count].astype(target.dtype)
        at += count


def unpack_columns(blocks, target, change=lambda part, first: part):
    for block in range(BLOCKS):
        target[block * LANES + COLS : (block + 1) * LANES, :] = jnp.zeros((LANES - COLS, LANES), target.dtype)
    for t in range(TPS):
        packed = blocks[t]
        store_rows(target, MAIN * t, change(packed, MAIN * t))
        store_rows(target, MAIN * t + 48, change(unfolded(packed), MAIN * t + 48))
    lane = lanes_of(8)
    for group in range(TPS // 4):
        parts = [
            pltpu.roll(blocks[4 * group + q, 32:40].astype(f32), PIECE * q + LANES - FREE, 1) for q in range(4)
        ]
        value = parts[3]
        for q in (2, 1, 0):
            value = jnp.where(lane < PIECE * (q + 1), parts[q], value)
        store_rows(target, SHARED + 8 * group, change(value, SHARED + 8 * group))


def unpack_rows(blocks, at, targets, change):
    for core in range(2):
        for z in range(DEPTH):
            b = place(core, z)
            packed = blocks[core, z]
            low = unfolded(packed)
            for first, part in ((0, packed), (WIDE, low[:8]), (MAIN, low[8:])):
                for target, value in zip(targets, change(part, first, b * COLS, packed)):
                    target[first : first + part.shape[0], b * LANES : (b + 1) * LANES] = value


def eye_of(at, first, count, col):
    row = at[0] if first < MAIN else at[1]
    return (rows_of(count) + (row + first) == lanes_of(count) + col) & (lanes_of(count) < COLS)


def own_eye(at):
    return jnp.concatenate([eye_of(at, 0, MAIN, at[2]), eye_of(at, MAIN, ROWS - MAIN, at[2])], axis=0)


def poly(eye, current):
    return jnp.where(eye, 1.5 - 0.5 * current, -0.5 * current)


def dot(left, right):
    return jnp.dot(left, right, preferred_element_type=f32)


def copies(out, value):
    value = value.astype(out.dtype)
    for i in range(out.shape[0]):
        out[i] = value


def send_tp(at, out, block, tail=None):
    copies(out, pack_tp(block[:MAIN], block[MAIN:ROWS], at[3], tail))


def gram_kernel(at, low, whole0, whole1, out, trace, own, share):
    mine = low[...]
    trace[...] = jnp.broadcast_to(jnp.sum(jnp.square(mine.astype(f32)), keepdims=True), trace.shape)
    own[:COLS] = mine
    own[COLS:] = jnp.zeros((LANES - COLS, own.shape[1]), bf16)
    half = D // 2
    for h, whole in enumerate((whole0, whole1)):
        share[h * half : (h + 1) * half] = lax.dot_general(
            whole[...], own[...], (((1,), (1,)), ((), ())), preferred_element_type=f32
        )
    for t in range(TPS):
        group, q = divmod(t, 4)
        shared = share[SHARED + 8 * group : SHARED + 8 * group + 8]
        out[t] = pack_tp(share[MAIN * t : MAIN * (t + 1)], shared, (FREE - PIECE * q) % LANES)


def total_kernel(trace, arrived, out):
    total = arrived[0]
    for t in range(1, TPS):
        total += arrived[t]
    spot = (rows_of(SENT) == SENT - 1) & (lanes_of(SENT) == FREE)
    copies(out, jnp.where(spot, trace[0:1], total))


def square_kernel(at, cols, out, whole):
    unpack_columns(cols, whole)
    ends = cols[0, SENT - 8 :]
    for t in range(1, TPS):
        ends += cols[t, SENT - 8 :]
    trace = jnp.sum(jnp.where((rows_of(8) == 7) & (lanes_of(8) == FREE), ends, 0.0), keepdims=True)
    square = jnp.zeros((LANES, LANES), f32)
    for block in range(BLOCKS):
        value = whole[block * LANES : (block + 1) * LANES, :]
        square += value * value
    square = jnp.sum(jnp.where(lanes_of(LANES) < COLS, square, 0.0), keepdims=True)

    def rows_at(first, count, target):
        for i in range(0, count, 8):
            block = (first + i) // COLS
            start = pl.multiple_of(block * LANES + (first + i) - block * COLS, 8)
            target.append(whole[pl.ds(start, 8), :])
        return target

    value = jnp.concatenate(rows_at(at[1] + MAIN, 8, rows_at(at[0], MAIN, [])), axis=0)
    row, lane = rows_of(WIDE - SPARE), lanes_of(WIDE - SPARE)
    tail = jnp.where((row == 0) & (lane == COLS), square, jnp.where((row == 0) & (lane == COLS + 1), trace, 0.0))
    copies(out, pack_z(value, tail))


def first_kernel(at, rows, cols, out, poly_rows, current_rows, spectral_out, right):
    tails = jnp.zeros((WIDE - SPARE, LANES), f32)
    for core in range(2):
        for z in range(DEPTH):
            tails += rows[core, z, SPARE:WIDE]
    spot = rows_of(WIDE - SPARE) == 0
    lane = lanes_of(WIDE - SPARE)
    square = jnp.sum(jnp.where(spot & (lane == COLS), tails, 0.0), keepdims=True)
    trace = jnp.sum(jnp.where(spot & (lane == COLS + 1), tails, 0.0), keepdims=True)
    spectral = 2.0 * square / (trace + EPS)
    inverse = 1.0 / spectral
    spectral_out[...] = jnp.broadcast_to(spectral, spectral_out.shape)

    def of_cols(part, first):
        n = part.shape[0]
        eye = rows_of(n) + first == lanes_of(n) + at[2]
        return poly(eye, part * inverse)

    unpack_columns(cols, right, of_cols)

    def of_rows(part, first, col, packed):
        current = part * inverse
        return (
            poly(eye_of(at, first, part.shape[0], col), current).astype(bf16),
            current.astype(bf16),
        )

    unpack_rows(rows, at, (poly_rows, current_rows), of_rows)
    send_tp(at, out, dot(poly_rows[...], right[...]))


def next_poly(at, current):
    eye = own_eye(at)
    return poly(eye, current), jnp.sum(jnp.where(eye, current, 0.0), axis=0, keepdims=True)


def second_kernel(at, current_rows, cols, out_cols, out_rows, right):
    unpack_columns(cols, right)
    value, diag = next_poly(at, dot(current_rows[...], right[...]))
    send_tp(at, out_cols, value)
    copies(out_rows, pack_z(value, spread(diag)))


def third_kernel(at, poly_rows, rows, cols, out_square, out_product, current_rows, first_rows, right):
    unpack_columns(cols, right)
    copies(out_product, pack_z(dot(poly_rows[...], right[...])))

    def of_rows(part, first, col, packed):
        eye = eye_of(at, first, part.shape[0], col)
        part = part.astype(f32)
        return part.astype(bf16), jnp.where(eye, gathered(packed), -2.0 * part).astype(bf16)

    unpack_rows(rows, at, (first_rows, current_rows), of_rows)
    send_tp(at, out_square, dot(first_rows[...], right[...]))


def fourth_kernel(at, current_rows, cols, out, right):
    unpack_columns(cols, right)
    send_tp(at, out, next_poly(at, dot(current_rows[...], right[...]))[0])


def fifth_kernel(at, rows, cols, out, product_rows, right):
    unpack_columns(cols, right)
    unpack_rows(rows, at, (product_rows,), lambda part, first, col, packed: (part.astype(bf16),))
    send_tp(at, out, dot(product_rows[...], right[...]))


def last_kernel(cols, out):
    unpack_columns(cols, out)


def call(kernel, outs, *args, scratch=()):
    vmem = pl.BlockSpec(memory_space=pltpu.VMEM)
    smem = pl.BlockSpec(memory_space=pltpu.SMEM)
    return pl.pallas_call(
        kernel,
        out_shape=[jax.ShapeDtypeStruct(shape, dtype) for shape, dtype in outs],
        in_specs=[smem if a.dtype == jnp.int32 else vmem for a in args],
        out_specs=[vmem] * len(outs),
        scratch_shapes=[pltpu.VMEM(shape, dtype) for shape, dtype in scratch],
        compiler_params=pltpu.CompilerParams(vmem_limit_bytes=24 * 2**20),
        name=kernel.__name__,
    )(*args)


def exchange(stacked, axes):
    return lax.all_to_all(stacked, axes, split_axis=0, concat_axis=0, tiled=True)


def both_cores(by_z):
    return lax.all_gather(by_z, "core")


def local(grad_gate, grad_up, moment_gate, moment_up):
    gate_next = BETA * moment_gate + grad_gate
    up_next = BETA * moment_up + grad_up
    half = gate_next.shape[1]
    low = jnp.concatenate([gate_next.astype(bf16), up_next.astype(bf16)], axis=1)
    low = jnp.pad(low, ((0, 0), (0, 3 * LANES - 2 * half)))
    z, core, t = lax.axis_index("z"), lax.axis_index("core"), lax.axis_index(TP)
    own = place(core, z)
    at = jnp.stack(
        [
            t * MAIN,
            SHARED + 8 * (t // 4) - MAIN,
            own * COLS,
            (FREE - PIECE * (t % 4)) % LANES,
            own * LANES,
        ]
    ).astype(jnp.int32)
    low, at = lax.optimization_barrier((low, at))
    by_z = lax.all_gather(low, "z")
    whole = [
        lax.all_gather(by_z[h * NEAR : (h + 1) * NEAR], "core").reshape(D // 2, -1) for h in range(2)
    ]

    right = ((KDIM, LANES), bf16)
    left = ((ROWS, KDIM), bf16)
    block = ((ROWS, LANES), f32)
    to_tp, to_z = ((TPS, SENT, LANES), bf16), ((DEPTH, WIDE, LANES), bf16)
    to_tp32, to_z32 = (to_tp[0], f32), (to_z[0], f32)

    shares, trace = call(
        gram_kernel,
        [to_tp32, ((8, LANES), f32)],
        at,
        low,
        *whole,
        scratch=[((LANES, low.shape[1]), bf16), ((D, LANES), f32)],
    )
    (cols,) = call(total_kernel, [to_tp32], trace, exchange(shares, TP))
    cols = exchange(cols, TP)
    (rows,) = call(square_kernel, [to_z32], at, cols, scratch=[(right[0], f32)])
    rows = both_cores(exchange(rows, "z"))
    sent, poly_rows, current_rows, spectral = call(
        first_kernel, [to_tp, left, left, ((8, LANES), f32)], at, rows, cols, scratch=[right]
    )
    cols, rows = call(second_kernel, [to_tp, to_z], at, current_rows, exchange(sent, TP), scratch=[right])
    cols = exchange(cols, TP)
    rows = both_cores(exchange(rows, "z"))
    square, product, current_rows = call(
        third_kernel, [to_tp, to_z, left], at, poly_rows, rows, cols, scratch=[left, right]
    )
    cols = exchange(square, TP)
    rows = both_cores(exchange(product, "z"))
    (cols,) = call(fourth_kernel, [to_tp], at, current_rows, cols, scratch=[right])
    cols = exchange(cols, TP)
    (cols,) = call(fifth_kernel, [to_tp], at, rows, cols, scratch=[left, right])
    (product,) = call(last_kernel, [right], exchange(cols, TP))

    whole_product = product.reshape(BLOCKS, LANES, LANES)[:, :COLS].reshape(2, D // 2, LANES)
    over_rows = (((0,), (0,)), ((), ()))
    ortho = sum(
        lax.dot_general(whole_product[h, :, :COLS], whole[h], over_rows, preferred_element_type=f32)
        for h in range(2)
    )
    ortho = ortho * jnp.sqrt(2.0 * FF / spectral[0, 0])
    return gate_next, up_next, ortho[:, :half], ortho[:, half : 2 * half]


def solution(mesh):
    split = Mesh(mesh.devices.reshape(DEPTH, 2, 8, 4), ("z", "core", "y", "x"))
    spec = P(FS, TP)
    return jax.shard_map(
        local, mesh=split, in_specs=(spec,) * 4, out_specs=(spec,) * 4, check_vma=False
    )
```

```python
import jax
import jax.numpy as jnp
from jax import lax
from jax.experimental import pallas as pl
from jax.experimental.pallas import tpu as pltpu
from jax.sharding import Mesh
from jax.sharding import PartitionSpec as P

FF = 5632
FS = ("z", "core")
TP = ("y", "x")
BETA = 0.95
EPS = 1e-06
LANES = 128
D = 2112
COLS = 88
BLOCKS = D // COLS
DEPTH = 12
NEAR = 6
TPS = 32
MAIN = 64
SHARED = TPS * MAIN
ROWS = MAIN + 8
PIECE = COLS // 4
SENT = 48
WIDE = 56
FREE = 96
SPARE = 48
KDIM = BLOCKS * LANES
f32, bf16 = jnp.float32, jnp.bfloat16


def place(core, z):
    return ((z // NEAR) * 2 + core) * NEAR + z % NEAR


def lanes_of(rows):
    return lax.broadcasted_iota(jnp.int32, (rows, LANES), 1)


def rows_of(rows):
    return lax.broadcasted_iota(jnp.int32, (rows, LANES), 0)


def folded(block, low):
    lane = lanes_of(16)
    return [
        jnp.where(lane < COLS, block[16 * i : 16 * i + 16], pltpu.roll(low, shift, 1))
        for i, shift in enumerate((COLS, COLS - 40, COLS - 80))
    ]


def unfolded(packed):
    lane = lanes_of(16)
    a, b, c = (
        pltpu.roll(packed[16 * i : 16 * i + 16].astype(f32), shift, 1)
        for i, shift in enumerate((40, 80, 120))
    )
    return jnp.where(lane < 40, a, jnp.where(lane < 80, b, c))


def pack_tp(main, shared, shift, tail=None):
    a, b, c = folded(main, main[48:64])
    top = jnp.where(lanes_of(8) < FREE, c[:8], pltpu.roll(shared, shift, 1))
    end = c[8:] if tail is None else jnp.where(lanes_of(8) < FREE, c[8:], tail)
    return jnp.concatenate([a, b, top, end], axis=0)


def pack_z(block, tail=None):
    end = block[SPARE:WIDE]
    if tail is not None:
        end = jnp.where(lanes_of(WIDE - SPARE) < COLS, end, tail)
    return jnp.concatenate([*folded(block, block[WIDE:ROWS]), end], axis=0)


def spread(row):
    row = jnp.broadcast_to(row, (WIDE - SPARE, LANES))
    at = rows_of(WIDE - SPARE)
    return jnp.where(
        at == 0,
        pltpu.roll(row, COLS, 1),
        jnp.where(at == 1, pltpu.roll(row, COLS - 40, 1), pltpu.roll(row, COLS - 80, 1)),
    )


def gathered(packed):
    tail = packed[SPARE:WIDE].astype(f32)
    lane = lanes_of(1)
    return jnp.where(
        lane < 40,
        pltpu.roll(tail, 40, 1)[0:1],
        jnp.where(lane < 80, pltpu.roll(tail, 80, 1)[1:2], pltpu.roll(tail, 120, 1)[2:3]),
    )


def store_rows(target, first, value):
    at, last = first, first + value.shape[0]
    while at < last:
        block, row = divmod(at, COLS)
        count = min(COLS - row, last - at)
        start = block * LANES + row
        target[start : start + count, :] = value[at - first : at - first + count].astype(target.dtype)
        at += count


def unpack_columns(blocks, target, change=lambda part, first: part):
    for block in range(BLOCKS):
        target[block * LANES + COLS : (block + 1) * LANES, :] = jnp.zeros((LANES - COLS, LANES), target.dtype)
    for t in range(TPS):
        packed = blocks[t]
        store_rows(target, MAIN * t, change(packed, MAIN * t))
        store_rows(target, MAIN * t + 48, change(unfolded(packed), MAIN * t + 48))
    lane = lanes_of(8)
    for group in range(TPS // 4):
        parts = [
            pltpu.roll(blocks[4 * group + q, 32:40].astype(f32), PIECE * q + LANES - FREE, 1) for q in range(4)
        ]
        value = parts[3]
        for q in (2, 1, 0):
            value = jnp.where(lane < PIECE * (q + 1), parts[q], value)
        store_rows(target, SHARED + 8 * group, change(value, SHARED + 8 * group))


def unpack_rows(blocks, at, targets, change):
    for core in range(2):
        for z in range(DEPTH):
            b = place(core, z)
            packed = blocks[core, z]
            low = unfolded(packed)
            for first, part in ((0, packed), (WIDE, low[:8]), (MAIN, low[8:])):
                for target, value in zip(targets, change(part, first, b * COLS, packed)):
                    target[first : first + part.shape[0], b * LANES : (b + 1) * LANES] = value


def eye_of(at, first, count, col):
    row = at[0] if first < MAIN else at[1]
    return (rows_of(count) + (row + first) == lanes_of(count) + col) & (lanes_of(count) < COLS)


def own_eye(at):
    return jnp.concatenate([eye_of(at, 0, MAIN, at[2]), eye_of(at, MAIN, ROWS - MAIN, at[2])], axis=0)


def poly(eye, current):
    return jnp.where(eye, 1.5 - 0.5 * current, -0.5 * current)


def dot(left, right):
    return jnp.dot(left, right, preferred_element_type=f32)


def copies(out, value):
    value = value.astype(out.dtype)
    for i in range(out.shape[0]):
        out[i] = value


def send_tp(at, out, block, tail=None):
    copies(out, pack_tp(block[:MAIN], block[MAIN:ROWS], at[3], tail))


def gram_kernel(at, low, whole0, whole1, out, trace, own, share):
    mine = low[...]
    trace[...] = jnp.broadcast_to(jnp.sum(jnp.square(mine.astype(f32)), keepdims=True), trace.shape)
    own[:COLS] = mine
    own[COLS:] = jnp.zeros((LANES - COLS, own.shape[1]), bf16)
    half = D // 2
    for h, whole in enumerate((whole0, whole1)):
        share[h * half : (h + 1) * half] = lax.dot_general(
            whole[...], own[...], (((1,), (1,)), ((), ())), preferred_element_type=f32
        )
    for t in range(TPS):
        group, q = divmod(t, 4)
        shared = share[SHARED + 8 * group : SHARED + 8 * group + 8]
        out[t] = pack_tp(share[MAIN * t : MAIN * (t + 1)], shared, (FREE - PIECE * q) % LANES)


def total_kernel(trace, arrived, out):
    total = arrived[0]
    for t in range(1, TPS):
        total += arrived[t]
    spot = (rows_of(SENT) == SENT - 1) & (lanes_of(SENT) == FREE)
    copies(out, jnp.where(spot, trace[0:1], total))


def square_kernel(at, cols, out, whole):
    unpack_columns(cols, whole)
    ends = cols[0, SENT - 8 :]
    for t in range(1, TPS):
        ends += cols[t, SENT - 8 :]
    trace = jnp.sum(jnp.where((rows_of(8) == 7) & (lanes_of(8) == FREE), ends, 0.0), keepdims=True)
    square = jnp.zeros((LANES, LANES), f32)
    for block in range(BLOCKS):
        value = whole[block * LANES : (block + 1) * LANES, :]
        square += value * value
    square = jnp.sum(jnp.where(lanes_of(LANES) < COLS, square, 0.0), keepdims=True)

    def rows_at(first, count, target):
        for i in range(0, count, 8):
            block = (first + i) // COLS
            start = pl.multiple_of(block * LANES + (first + i) - block * COLS, 8)
            target.append(whole[pl.ds(start, 8), :])
        return target

    value = jnp.concatenate(rows_at(at[1] + MAIN, 8, rows_at(at[0], MAIN, [])), axis=0)
    row, lane = rows_of(WIDE - SPARE), lanes_of(WIDE - SPARE)
    tail = jnp.where((row == 0) & (lane == COLS), square, jnp.where((row == 0) & (lane == COLS + 1), trace, 0.0))
    copies(out, pack_z(value, tail))


def first_kernel(at, rows, cols, out, poly_rows, current_rows, spectral_out, right):
    tails = jnp.zeros((WIDE - SPARE, LANES), f32)
    for core in range(2):
        for z in range(DEPTH):
            tails += rows[core, z, SPARE:WIDE]
    spot = rows_of(WIDE - SPARE) == 0
    lane = lanes_of(WIDE - SPARE)
    square = jnp.sum(jnp.where(spot & (lane == COLS), tails, 0.0), keepdims=True)
    trace = jnp.sum(jnp.where(spot & (lane == COLS + 1), tails, 0.0), keepdims=True)
    spectral = 2.0 * square / (trace + EPS)
    inverse = 1.0 / spectral
    spectral_out[...] = jnp.broadcast_to(spectral, spectral_out.shape)

    def of_cols(part, first):
        n = part.shape[0]
        eye = rows_of(n) + first == lanes_of(n) + at[2]
        return poly(eye, part * inverse)

    unpack_columns(cols, right, of_cols)

    def of_rows(part, first, col, packed):
        current = part * inverse
        return (
            poly(eye_of(at, first, part.shape[0], col), current).astype(bf16),
            current.astype(bf16),
        )

    unpack_rows(rows, at, (poly_rows, current_rows), of_rows)
    send_tp(at, out, dot(poly_rows[...], right[...]))


def next_poly(at, current):
    eye = own_eye(at)
    return poly(eye, current), jnp.sum(jnp.where(eye, current, 0.0), axis=0, keepdims=True)


def second_kernel(at, current_rows, cols, out_cols, out_rows, right):
    unpack_columns(cols, right)
    value, diag = next_poly(at, dot(current_rows[...], right[...]))
    send_tp(at, out_cols, value)
    copies(out_rows, pack_z(value, spread(diag)))


def third_kernel(at, poly_rows, rows, cols, out, right, kept, rows_kept, first_rows, current_rows):
    unpack_columns(cols, right)
    diagonal = [jnp.zeros((count, LANES), f32) for count in (WIDE, 8, 8)]

    def of_rows(part, first, col, packed):
        eye = eye_of(at, first, part.shape[0], col)
        i = (0, WIDE, MAIN).index(first)
        part = part.astype(f32)
        row = gathered(packed)
        diagonal[i] += jnp.where(eye, row, 0.0)
        return part.astype(bf16), jnp.where(eye, row, -2.0 * part).astype(bf16)

    unpack_rows(rows, at, (first_rows, current_rows), of_rows)
    own = pl.ds(pl.multiple_of(at[4], LANES), LANES)
    product = dot(poly_rows[...], right[...])
    moved = dot(current_rows[...], right[...])
    moved_low = moved.astype(bf16).astype(f32)
    square = dot(first_rows[...], right[...])
    moved_off = moved - moved_low
    kept[0] = first_rows[:, own].astype(f32)
    kept[1] = current_rows[:, own].astype(f32)
    kept[2] = moved_off
    kept[3] = square.astype(bf16).astype(f32) - square
    kept[4] = jnp.broadcast_to(
        jnp.sum(jnp.concatenate(diagonal, axis=0), axis=1, keepdims=True), (ROWS, LANES)
    )
    eye = own_eye(at)
    tail = spread(jnp.sum(jnp.where(eye, moved_off, 0.0), axis=0, keepdims=True))
    product, moved_low = pack_z(product).astype(bf16), pack_z(moved_low, tail).astype(bf16)
    for z in range(DEPTH):
        out[z, :WIDE] = product
        out[z, WIDE:] = moved_low
    mine = right[own, :].astype(f32)
    total = jnp.zeros((LANES, LANES), f32)
    for block in range(BLOCKS):
        value = right[block * LANES : (block + 1) * LANES, :].astype(f32)
        total += value * value
    total = jnp.sum(total, axis=0, keepdims=True)
    on = rows_of(LANES) == lanes_of(LANES)
    row = rows_of(8)
    rows_kept[...] = jnp.where(
        row == 0,
        jnp.sum(jnp.where(on, mine, 0.0), axis=0, keepdims=True),
        total.astype(bf16).astype(f32) - total,
    )


def fourth_kernel(at, rows, right, kept, rows_kept, out, product_rows, moved_rows):
    diagonal = [jnp.zeros((count, LANES), f32) for count in (WIDE, 8, 8)]

    def of_rows(part, first, col, packed):
        eye = eye_of(at, first, part.shape[0], col)
        diagonal[(0, WIDE, MAIN).index(first)] += jnp.where(eye, gathered(packed), 0.0)
        return (part.astype(bf16),)

    unpack_rows(rows.at[:, :, WIDE:], at, (moved_rows,), of_rows)
    unpack_rows(rows.at[:, :, :WIDE], at, (product_rows,), lambda part, first, col, packed: (part.astype(bf16),))
    moved_diagonal = jnp.sum(jnp.concatenate(diagonal, axis=0), axis=1, keepdims=True)
    poly_own, current_own, moved_off, square_off, current_diagonal = (kept[i] for i in range(5))
    poly_diagonal, square_diagonal = rows_kept[0:1], rows_kept[1:2]
    eye = own_eye(at)
    off = jnp.where(
        eye,
        moved_off * poly_own + current_own * square_off,
        moved_diagonal * poly_own
        + moved_off * poly_diagonal
        + current_diagonal * square_off
        + current_own * square_diagonal,
    )
    send_tp(at, out, poly(eye, dot(moved_rows[...], right[...]) + off))


def fifth_kernel(at, product_rows, cols, out, right):
    unpack_columns(cols, right)
    send_tp(at, out, dot(product_rows[...], right[...]))


def last_kernel(cols, out):
    unpack_columns(cols, out)


def call(kernel, outs, *args, scratch=()):
    vmem = pl.BlockSpec(memory_space=pltpu.VMEM)
    smem = pl.BlockSpec(memory_space=pltpu.SMEM)
    return pl.pallas_call(
        kernel,
        out_shape=[jax.ShapeDtypeStruct(shape, dtype) for shape, dtype in outs],
        in_specs=[smem if a.dtype == jnp.int32 else vmem for a in args],
        out_specs=[vmem] * len(outs),
        scratch_shapes=[pltpu.VMEM(shape, dtype) for shape, dtype in scratch],
        compiler_params=pltpu.CompilerParams(vmem_limit_bytes=24 * 2**20),
        name=kernel.__name__,
    )(*args)


def exchange(stacked, axes):
    return lax.all_to_all(stacked, axes, split_axis=0, concat_axis=0, tiled=True)


def both_cores(by_z):
    return lax.all_gather(by_z, "core")


def local(grad_gate, grad_up, moment_gate, moment_up):
    gate_next = BETA * moment_gate + grad_gate
    up_next = BETA * moment_up + grad_up
    half = gate_next.shape[1]
    low = jnp.concatenate([gate_next.astype(bf16), up_next.astype(bf16)], axis=1)
    low = jnp.pad(low, ((0, 0), (0, 3 * LANES - 2 * half)))
    z, core, t = lax.axis_index("z"), lax.axis_index("core"), lax.axis_index(TP)
    own = place(core, z)
    at = jnp.stack(
        [
            t * MAIN,
            SHARED + 8 * (t // 4) - MAIN,
            own * COLS,
            (FREE - PIECE * (t % 4)) % LANES,
            own * LANES,
        ]
    ).astype(jnp.int32)
    low, at = lax.optimization_barrier((low, at))
    by_z = lax.all_gather(low, "z")
    whole = [
        lax.all_gather(by_z[h * NEAR : (h + 1) * NEAR], "core").reshape(D // 2, -1) for h in range(2)
    ]

    right = ((KDIM, LANES), bf16)
    left = ((ROWS, KDIM), bf16)
    block = ((ROWS, LANES), f32)
    to_tp, to_z = ((TPS, SENT, LANES), bf16), ((DEPTH, WIDE, LANES), bf16)
    to_tp32, to_z32 = (to_tp[0], f32), (to_z[0], f32)

    shares, trace = call(
        gram_kernel,
        [to_tp32, ((8, LANES), f32)],
        at,
        low,
        *whole,
        scratch=[((LANES, low.shape[1]), bf16), ((D, LANES), f32)],
    )
    (cols,) = call(total_kernel, [to_tp32], trace, exchange(shares, TP))
    cols = exchange(cols, TP)
    (rows,) = call(square_kernel, [to_z32], at, cols, scratch=[(right[0], f32)])
    rows = both_cores(exchange(rows, "z"))
    sent, poly_rows, current_rows, spectral = call(
        first_kernel, [to_tp, left, left, ((8, LANES), f32)], at, rows, cols, scratch=[right]
    )
    cols, rows = call(second_kernel, [to_tp, to_z], at, current_rows, exchange(sent, TP), scratch=[right])
    rows = both_cores(exchange(rows, "z"))
    cols = exchange(cols, TP)
    rows, right_poly, kept, rows_kept = call(
        third_kernel,
        [((DEPTH, 2 * WIDE, LANES), bf16), right, ((5, ROWS, LANES), f32), ((8, LANES), f32)],
        at,
        poly_rows,
        rows,
        cols,
        scratch=[left, left],
    )
    rows = both_cores(exchange(rows, "z"))
    cols, product_rows = call(
        fourth_kernel, [to_tp, left], at, rows, right_poly, kept, rows_kept, scratch=[left]
    )
    (cols,) = call(fifth_kernel, [to_tp], at, product_rows, exchange(cols, TP), scratch=[right])
    (product,) = call(last_kernel, [right], exchange(cols, TP))

    whole_product = product.reshape(BLOCKS, LANES, LANES)[:, :COLS].reshape(2, D // 2, LANES)
    over_rows = (((0,), (0,)), ((), ()))
    ortho = sum(
        lax.dot_general(whole_product[h, :, :COLS], whole[h], over_rows, preferred_element_type=f32)
        for h in range(2)
    )
    ortho = ortho * jnp.sqrt(2.0 * FF / spectral[0, 0])
    return gate_next, up_next, ortho[:, :half], ortho[:, half : 2 * half]


def solution(mesh):
    split = Mesh(mesh.devices.reshape(DEPTH, 2, 8, 4), ("z", "core", "y", "x"))
    spec = P(FS, TP)
    return jax.shard_map(
        local, mesh=split, in_specs=(spec,) * 4, out_specs=(spec,) * 4, check_vma=False
    )
```

```python
import jax
import jax.numpy as jnp
from jax import lax
from jax.experimental import pallas as pl
from jax.experimental.pallas import tpu as pltpu
from jax.sharding import Mesh
from jax.sharding import PartitionSpec as P

FF = 5632
FS = ("z", "core")
TP = ("y", "x")
BETA = 0.95
EPS = 1e-06
LANES = 128
D = 2112
COLS = 88
BLOCKS = D // COLS
DEPTH = 12
NEAR = 6
TPS = 32
MAIN = 64
SHARED = TPS * MAIN
ROWS = MAIN + 8
PIECE = COLS // 4
SENT = 48
WIDE = 56
FREE = 96
SPARE = 48
KDIM = BLOCKS * LANES
f32, bf16 = jnp.float32, jnp.bfloat16


def place(core, z):
    return ((z // NEAR) * 2 + core) * NEAR + z % NEAR


def lanes_of(rows):
    return lax.broadcasted_iota(jnp.int32, (rows, LANES), 1)


def rows_of(rows):
    return lax.broadcasted_iota(jnp.int32, (rows, LANES), 0)


def folded(block, low):
    lane = lanes_of(16)
    return [
        jnp.where(lane < COLS, block[16 * i : 16 * i + 16], pltpu.roll(low, shift, 1))
        for i, shift in enumerate((COLS, COLS - 40, COLS - 80))
    ]


def unfolded(packed):
    lane = lanes_of(16)
    a, b, c = (
        pltpu.roll(packed[16 * i : 16 * i + 16].astype(f32), shift, 1)
        for i, shift in enumerate((40, 80, 120))
    )
    return jnp.where(lane < 40, a, jnp.where(lane < 80, b, c))


def pack_tp(main, shared, shift, tail=None):
    a, b, c = folded(main, main[48:64])
    top = jnp.where(lanes_of(8) < FREE, c[:8], pltpu.roll(shared, shift, 1))
    end = c[8:] if tail is None else jnp.where(lanes_of(8) < FREE, c[8:], tail)
    return jnp.concatenate([a, b, top, end], axis=0)


def pack_z(block, tail=None):
    end = block[SPARE:WIDE]
    if tail is not None:
        end = jnp.where(lanes_of(WIDE - SPARE) < COLS, end, tail)
    return jnp.concatenate([*folded(block, block[WIDE:ROWS]), end], axis=0)


def spread(row):
    row = jnp.broadcast_to(row, (WIDE - SPARE, LANES))
    at = rows_of(WIDE - SPARE)
    return jnp.where(
        at == 0,
        pltpu.roll(row, COLS, 1),
        jnp.where(at == 1, pltpu.roll(row, COLS - 40, 1), pltpu.roll(row, COLS - 80, 1)),
    )


def gathered(packed):
    tail = packed[SPARE:WIDE].astype(f32)
    lane = lanes_of(1)
    return jnp.where(
        lane < 40,
        pltpu.roll(tail, 40, 1)[0:1],
        jnp.where(lane < 80, pltpu.roll(tail, 80, 1)[1:2], pltpu.roll(tail, 120, 1)[2:3]),
    )


def store_rows(target, first, value):
    at, last = first, first + value.shape[0]
    while at < last:
        block, row = divmod(at, COLS)
        count = min(COLS - row, last - at)
        start = block * LANES + row
        target[start : start + count, :] = value[at - first : at - first + count].astype(target.dtype)
        at += count


def unpack_columns(blocks, target, change=lambda part, first: part):
    for block in range(BLOCKS):
        target[block * LANES + COLS : (block + 1) * LANES, :] = jnp.zeros((LANES - COLS, LANES), target.dtype)
    for t in range(TPS):
        packed = blocks[t]
        store_rows(target, MAIN * t, change(packed, MAIN * t))
        store_rows(target, MAIN * t + 48, change(unfolded(packed), MAIN * t + 48))
    lane = lanes_of(8)
    for group in range(TPS // 4):
        parts = [
            pltpu.roll(blocks[4 * group + q, 32:40].astype(f32), PIECE * q + LANES - FREE, 1) for q in range(4)
        ]
        value = parts[3]
        for q in (2, 1, 0):
            value = jnp.where(lane < PIECE * (q + 1), parts[q], value)
        store_rows(target, SHARED + 8 * group, change(value, SHARED + 8 * group))


def unpack_rows(blocks, at, targets, change):
    for core in range(2):
        for z in range(DEPTH):
            b = place(core, z)
            packed = blocks[core, z]
            low = unfolded(packed)
            for first, part in ((0, packed), (WIDE, low[:8]), (MAIN, low[8:])):
                for target, value in zip(targets, change(part, first, b * COLS, packed)):
                    target[first : first + part.shape[0], b * LANES : (b + 1) * LANES] = value


def position():
    own = place(lax.axis_index("core"), lax.axis_index("z"))
    t = lax.axis_index("y") * 4 + lax.axis_index("x")
    return (
        t * MAIN,
        SHARED + 8 * (t // 4) - MAIN,
        own * COLS,
        (FREE + LANES - PIECE * (t % 4)) % LANES,
        own * LANES,
    )


def eye_of(at, first, count, col):
    row = at[0] if first < MAIN else at[1]
    return (rows_of(count) + (row + first) == lanes_of(count) + col) & (lanes_of(count) < COLS)


def own_eye(at):
    return jnp.concatenate([eye_of(at, 0, MAIN, at[2]), eye_of(at, MAIN, ROWS - MAIN, at[2])], axis=0)


def poly(eye, current):
    return jnp.where(eye, 1.5 - 0.5 * current, -0.5 * current)


def dot(left, right):
    return jnp.dot(left, right, preferred_element_type=f32)


def copies(out, value):
    value = value.astype(out.dtype)
    for i in range(out.shape[0]):
        out[i] = value


def send_tp(at, out, block, tail=None):
    copies(out, pack_tp(block[:MAIN], block[MAIN:ROWS], at[3], tail))


def gram_kernel(low, whole0, whole1, out, trace, own, share):
    mine = low[...]
    trace[...] = jnp.broadcast_to(jnp.sum(jnp.square(mine.astype(f32)), keepdims=True), trace.shape)
    own[:COLS] = mine
    own[COLS:] = jnp.zeros((LANES - COLS, own.shape[1]), bf16)
    half = D // 2
    for h, whole in enumerate((whole0, whole1)):
        share[h * half : (h + 1) * half] = lax.dot_general(
            whole[...], own[...], (((1,), (1,)), ((), ())), preferred_element_type=f32
        )
    for t in range(TPS):
        group, q = divmod(t, 4)
        shared = share[SHARED + 8 * group : SHARED + 8 * group + 8]
        out[t] = pack_tp(share[MAIN * t : MAIN * (t + 1)], shared, (FREE - PIECE * q) % LANES)


def total_kernel(trace, arrived, out):
    total = arrived[0]
    for t in range(1, TPS):
        total += arrived[t]
    spot = (rows_of(SENT) == SENT - 1) & (lanes_of(SENT) == FREE)
    copies(out, jnp.where(spot, trace[0:1], total))


def square_kernel(cols, out, whole):
    at = position()
    unpack_columns(cols, whole)
    ends = cols[0, SENT - 8 :]
    for t in range(1, TPS):
        ends += cols[t, SENT - 8 :]
    trace = jnp.sum(jnp.where((rows_of(8) == 7) & (lanes_of(8) == FREE), ends, 0.0), keepdims=True)
    square = jnp.zeros((LANES, LANES), f32)
    for block in range(BLOCKS):
        value = whole[block * LANES : (block + 1) * LANES, :]
        square += value * value
    square = jnp.sum(jnp.where(lanes_of(LANES) < COLS, square, 0.0), keepdims=True)

    def rows_at(first, count, target):
        for i in range(0, count, 8):
            block = (first + i) // COLS
            start = pl.multiple_of(block * LANES + (first + i) - block * COLS, 8)
            target.append(whole[pl.ds(start, 8), :])
        return target

    value = jnp.concatenate(rows_at(at[1] + MAIN, 8, rows_at(at[0], MAIN, [])), axis=0)
    row, lane = rows_of(WIDE - SPARE), lanes_of(WIDE - SPARE)
    tail = jnp.where((row == 0) & (lane == COLS), square, jnp.where((row == 0) & (lane == COLS + 1), trace, 0.0))
    copies(out, pack_z(value, tail))


def first_kernel(rows, cols, out, poly_rows, current_rows, spectral_out, right):
    at = position()
    tails = jnp.zeros((WIDE - SPARE, LANES), f32)
    for core in range(2):
        for z in range(DEPTH):
            tails += rows[core, z, SPARE:WIDE]
    spot = rows_of(WIDE - SPARE) == 0
    lane = lanes_of(WIDE - SPARE)
    square = jnp.sum(jnp.where(spot & (lane == COLS), tails, 0.0), keepdims=True)
    trace = jnp.sum(jnp.where(spot & (lane == COLS + 1), tails, 0.0), keepdims=True)
    spectral = 2.0 * square / (trace + EPS)
    inverse = 1.0 / spectral
    spectral_out[...] = jnp.broadcast_to(spectral, spectral_out.shape)

    def of_cols(part, first):
        n = part.shape[0]
        eye = rows_of(n) + first == lanes_of(n) + at[2]
        return poly(eye, part * inverse)

    unpack_columns(cols, right, of_cols)

    def of_rows(part, first, col, packed):
        current = part * inverse
        return (
            poly(eye_of(at, first, part.shape[0], col), current).astype(bf16),
            current.astype(bf16),
        )

    unpack_rows(rows, at, (poly_rows, current_rows), of_rows)
    send_tp(at, out, dot(poly_rows[...], right[...]))


def next_poly(at, current):
    eye = own_eye(at)
    return poly(eye, current), jnp.sum(jnp.where(eye, current, 0.0), axis=0, keepdims=True)


def second_kernel(current_rows, cols, out_cols, out_rows, right):
    at = position()
    unpack_columns(cols, right)
    value, diag = next_poly(at, dot(current_rows[...], right[...]))
    send_tp(at, out_cols, value)
    copies(out_rows, pack_z(value, spread(diag)))


def third_kernel(poly_rows, rows, cols, out, right, kept, rows_kept, first_rows, current_rows):
    at = position()
    unpack_columns(cols, right)
    diagonal = [jnp.zeros((count, LANES), f32) for count in (WIDE, 8, 8)]

    def of_rows(part, first, col, packed):
        eye = eye_of(at, first, part.shape[0], col)
        i = (0, WIDE, MAIN).index(first)
        part = part.astype(f32)
        row = gathered(packed)
        diagonal[i] += jnp.where(eye, row, 0.0)
        return part.astype(bf16), jnp.where(eye, row, -2.0 * part).astype(bf16)

    unpack_rows(rows, at, (first_rows, current_rows), of_rows)
    own = pl.ds(pl.multiple_of(at[4], LANES), LANES)
    product = dot(poly_rows[...], right[...])
    moved = dot(current_rows[...], right[...])
    moved_low = moved.astype(bf16).astype(f32)
    square = dot(first_rows[...], right[...])
    moved_off = moved - moved_low
    kept[0] = first_rows[:, own].astype(f32)
    kept[1] = current_rows[:, own].astype(f32)
    kept[2] = moved_off
    kept[3] = square.astype(bf16).astype(f32) - square
    kept[4] = jnp.broadcast_to(
        jnp.sum(jnp.concatenate(diagonal, axis=0), axis=1, keepdims=True), (ROWS, LANES)
    )
    eye = own_eye(at)
    tail = spread(jnp.sum(jnp.where(eye, moved_off, 0.0), axis=0, keepdims=True))
    product, moved_low = pack_z(product).astype(bf16), pack_z(moved_low, tail).astype(bf16)
    for z in range(DEPTH):
        out[z, :WIDE] = product
        out[z, WIDE:] = moved_low
    mine = right[own, :].astype(f32)
    total = jnp.zeros((LANES, LANES), f32)
    for block in range(BLOCKS):
        value = right[block * LANES : (block + 1) * LANES, :].astype(f32)
        total += value * value
    total = jnp.sum(total, axis=0, keepdims=True)
    on = rows_of(LANES) == lanes_of(LANES)
    row = rows_of(8)
    rows_kept[...] = jnp.where(
        row == 0,
        jnp.sum(jnp.where(on, mine, 0.0), axis=0, keepdims=True),
        total.astype(bf16).astype(f32) - total,
    )


def fourth_kernel(rows, right, kept, rows_kept, out, product_rows, moved_rows):
    at = position()
    diagonal = [jnp.zeros((count, LANES), f32) for count in (WIDE, 8, 8)]

    def of_rows(part, first, col, packed):
        eye = eye_of(at, first, part.shape[0], col)
        diagonal[(0, WIDE, MAIN).index(first)] += jnp.where(eye, gathered(packed), 0.0)
        return (part.astype(bf16),)

    unpack_rows(rows.at[:, :, WIDE:], at, (moved_rows,), of_rows)
    unpack_rows(rows.at[:, :, :WIDE], at, (product_rows,), lambda part, first, col, packed: (part.astype(bf16),))
    moved_diagonal = jnp.sum(jnp.concatenate(diagonal, axis=0), axis=1, keepdims=True)
    poly_own, current_own, moved_off, square_off, current_diagonal = (kept[i] for i in range(5))
    poly_diagonal, square_diagonal = rows_kept[0:1], rows_kept[1:2]
    eye = own_eye(at)
    off = jnp.where(
        eye,
        moved_off * poly_own + current_own * square_off,
        moved_diagonal * poly_own
        + moved_off * poly_diagonal
        + current_diagonal * square_off
        + current_own * square_diagonal,
    )
    send_tp(at, out, poly(eye, dot(moved_rows[...], right[...]) + off))


def fifth_kernel(product_rows, cols, out, right):
    at = position()
    unpack_columns(cols, right)
    send_tp(at, out, dot(product_rows[...], right[...]))


def last_kernel(cols, out):
    unpack_columns(cols, out)


def call(kernel, outs, *args, scratch=()):
    vmem = pl.BlockSpec(memory_space=pltpu.VMEM)
    return pl.pallas_call(
        kernel,
        out_shape=[jax.ShapeDtypeStruct(shape, dtype) for shape, dtype in outs],
        in_specs=[vmem] * len(args),
        out_specs=[vmem] * len(outs),
        scratch_shapes=[pltpu.VMEM(shape, dtype) for shape, dtype in scratch],
        compiler_params=pltpu.CompilerParams(vmem_limit_bytes=24 * 2**20),
        name=kernel.__name__,
    )(*args)


def exchange(stacked, axes):
    return lax.all_to_all(stacked, axes, split_axis=0, concat_axis=0, tiled=True)


def both_cores(by_z):
    return lax.all_gather(by_z, "core")


def local(grad_gate, grad_up, moment_gate, moment_up):
    gate_next = BETA * moment_gate + grad_gate
    up_next = BETA * moment_up + grad_up
    half = gate_next.shape[1]
    low = jnp.concatenate([gate_next.astype(bf16), up_next.astype(bf16)], axis=1)
    low = jnp.pad(low, ((0, 0), (0, 3 * LANES - 2 * half)))
    by_z = lax.all_gather(low, "z")
    whole = [
        lax.all_gather(by_z[h * NEAR : (h + 1) * NEAR], "core").reshape(D // 2, -1) for h in range(2)
    ]

    right = ((KDIM, LANES), bf16)
    left = ((ROWS, KDIM), bf16)
    block = ((ROWS, LANES), f32)
    to_tp, to_z = ((TPS, SENT, LANES), bf16), ((DEPTH, WIDE, LANES), bf16)
    to_tp32, to_z32 = (to_tp[0], f32), (to_z[0], f32)

    shares, trace = call(
        gram_kernel,
        [to_tp32, ((8, LANES), f32)],
        low,
        *whole,
        scratch=[((LANES, low.shape[1]), bf16), ((D, LANES), f32)],
    )
    (cols,) = call(total_kernel, [to_tp32], trace, exchange(shares, TP))
    cols = exchange(cols, TP)
    (rows,) = call(square_kernel, [to_z32], cols, scratch=[(right[0], f32)])
    rows = both_cores(exchange(rows, "z"))
    sent, poly_rows, current_rows, spectral = call(
        first_kernel, [to_tp, left, left, ((8, LANES), f32)], rows, cols, scratch=[right]
    )
    cols, rows = call(second_kernel, [to_tp, to_z], current_rows, exchange(sent, TP), scratch=[right])
    rows = both_cores(exchange(rows, "z"))
    cols = exchange(cols, TP)
    rows, right_poly, kept, rows_kept = call(
        third_kernel,
        [((DEPTH, 2 * WIDE, LANES), bf16), right, ((5, ROWS, LANES), f32), ((8, LANES), f32)],
        poly_rows,
        rows,
        cols,
        scratch=[left, left],
    )
    rows = both_cores(exchange(rows, "z"))
    cols, product_rows = call(
        fourth_kernel, [to_tp, left], rows, right_poly, kept, rows_kept, scratch=[left]
    )
    (cols,) = call(fifth_kernel, [to_tp], product_rows, exchange(cols, TP), scratch=[right])
    (product,) = call(last_kernel, [right], exchange(cols, TP))

    whole_product = product.reshape(BLOCKS, LANES, LANES)[:, :COLS].reshape(2, D // 2, LANES)
    over_rows = (((0,), (0,)), ((), ()))
    ortho = sum(
        lax.dot_general(whole_product[h, :, :COLS], whole[h], over_rows, preferred_element_type=f32)
        for h in range(2)
    )
    ortho = ortho * jnp.sqrt(2.0 * FF / spectral[0, 0])
    return gate_next, up_next, ortho[:, :half], ortho[:, half : 2 * half]


def solution(mesh):
    split = Mesh(mesh.devices.reshape(DEPTH, 2, 8, 4), ("z", "core", "y", "x"))
    spec = P(FS, TP)
    return jax.shard_map(
        local, mesh=split, in_specs=(spec,) * 4, out_specs=(spec,) * 4, check_vma=False
    )
```

```python
import jax
import jax.numpy as jnp
from jax import lax
from jax.experimental import pallas as pl
from jax.experimental.pallas import tpu as pltpu
from jax.sharding import Mesh
from jax.sharding import PartitionSpec as P

FF = 5632
FS = ("z", "core")
TP = ("y", "x")
BETA = 0.95
EPS = 1e-06
LANES = 128
D = 2112
COLS = 88
BLOCKS = D // COLS
DEPTH = 12
NEAR = 6
TPS = 32
MAIN = 64
SHARED = TPS * MAIN
ROWS = MAIN + 8
PIECE = COLS // 4
SENT = 48
WIDE = 56
FREE = 96
SPARE = 48
KDIM = BLOCKS * LANES
f32, bf16 = jnp.float32, jnp.bfloat16


def place(core, z):
    return ((z // NEAR) * 2 + core) * NEAR + z % NEAR


def lanes_of(rows):
    return lax.broadcasted_iota(jnp.int32, (rows, LANES), 1)


def rows_of(rows):
    return lax.broadcasted_iota(jnp.int32, (rows, LANES), 0)


def folded(block, low):
    lane = lanes_of(16)
    return [
        jnp.where(lane < COLS, block[16 * i : 16 * i + 16], pltpu.roll(low, shift, 1))
        for i, shift in enumerate((COLS, COLS - 40, COLS - 80))
    ]


def unfolded(packed):
    lane = lanes_of(16)
    a, b, c = (
        pltpu.roll(packed[16 * i : 16 * i + 16].astype(f32), shift, 1)
        for i, shift in enumerate((40, 80, 120))
    )
    return jnp.where(lane < 40, a, jnp.where(lane < 80, b, c))


def pack_tp(main, shared, shift, tail=None):
    a, b, c = folded(main, main[48:64])
    top = jnp.where(lanes_of(8) < FREE, c[:8], pltpu.roll(shared, shift, 1))
    end = c[8:] if tail is None else jnp.where(lanes_of(8) < FREE, c[8:], tail)
    return jnp.concatenate([a, b, top, end], axis=0)


def pack_z(block, tail=None):
    end = block[SPARE:WIDE]
    if tail is not None:
        end = jnp.where(lanes_of(WIDE - SPARE) < COLS, end, tail)
    return jnp.concatenate([*folded(block, block[WIDE:ROWS]), end], axis=0)


def spread(row):
    row = jnp.broadcast_to(row, (WIDE - SPARE, LANES))
    at = rows_of(WIDE - SPARE)
    return jnp.where(
        at == 0,
        pltpu.roll(row, COLS, 1),
        jnp.where(at == 1, pltpu.roll(row, COLS - 40, 1), pltpu.roll(row, COLS - 80, 1)),
    )


def gathered(packed):
    tail = packed[SPARE:WIDE].astype(f32)
    lane = lanes_of(1)
    return jnp.where(
        lane < 40,
        pltpu.roll(tail, 40, 1)[0:1],
        jnp.where(lane < 80, pltpu.roll(tail, 80, 1)[1:2], pltpu.roll(tail, 120, 1)[2:3]),
    )


def store_rows(target, first, value):
    at, last = first, first + value.shape[0]
    while at < last:
        block, row = divmod(at, COLS)
        count = min(COLS - row, last - at)
        start = block * LANES + row
        target[start : start + count, :] = value[at - first : at - first + count].astype(target.dtype)
        at += count


def unpack_columns(blocks, target, scales=None):
    def scaled(part, t):
        return part if scales is None else part * scales[t]

    for block in range(BLOCKS):
        target[block * LANES + COLS : (block + 1) * LANES, :] = jnp.zeros((LANES - COLS, LANES), target.dtype)
    for t in range(TPS):
        packed = blocks[t]
        store_rows(target, MAIN * t, scaled(packed, t))
        store_rows(target, MAIN * t + 48, scaled(unfolded(packed), t))
    lane = lanes_of(8)
    for group in range(TPS // 4):
        parts = [
            scaled(
                pltpu.roll(blocks[4 * group + q, 32:40].astype(f32), PIECE * q + LANES - FREE, 1), 4 * group + q
            )
            for q in range(4)
        ]
        value = parts[3]
        for q in (2, 1, 0):
            value = jnp.where(lane < PIECE * (q + 1), parts[q], value)
        store_rows(target, SHARED + 8 * group, value)


def unpack_rows(blocks, at, targets, change):
    for core in range(2):
        for z in range(DEPTH):
            b = place(core, z)
            packed = blocks[core, z]
            low = unfolded(packed)
            for first, part in ((0, packed), (WIDE, low[:8]), (MAIN, low[8:])):
                for target, value in zip(targets, change(part, first, b * COLS, packed)):
                    target[first : first + part.shape[0], b * LANES : (b + 1) * LANES] = value


def position():
    own = place(lax.axis_index("core"), lax.axis_index("z"))
    t = lax.axis_index("y") * 4 + lax.axis_index("x")
    return (
        t * MAIN,
        SHARED + 8 * (t // 4) - MAIN,
        own * COLS,
        (FREE + LANES - PIECE * (t % 4)) % LANES,
        own * LANES,
        t % 4,
    )


def eye_of(at, first, count, col):
    row = at[0] if first < MAIN else at[1]
    return (rows_of(count) + (row + first) == lanes_of(count) + col) & (lanes_of(count) < COLS)


def own_eye(at):
    return jnp.concatenate([eye_of(at, 0, MAIN, at[2]), eye_of(at, MAIN, ROWS - MAIN, at[2])], axis=0)


def poly(eye, current):
    return jnp.where(eye, 1.5 - 0.5 * current, -0.5 * current)


def dot(left, right):
    return jnp.dot(left, right, preferred_element_type=f32)


def copies(out, value):
    value = value.astype(out.dtype)
    for i in range(out.shape[0]):
        out[i] = value


def send_tp(at, out, block, tail=None):
    copies(out, pack_tp(block[:MAIN], block[MAIN:ROWS], at[3], tail))


def gram_kernel(low, whole0, whole1, out, own, share):
    own[:COLS] = low[...]
    own[COLS:] = jnp.zeros((LANES - COLS, own.shape[1]), bf16)
    half = D // 2
    for h, whole in enumerate((whole0, whole1)):
        share[h * half : (h + 1) * half] = lax.dot_general(
            whole[...], own[...], (((1,), (1,)), ((), ())), preferred_element_type=f32
        )
    for t in range(TPS):
        group, q = divmod(t, 4)
        shared = share[SHARED + 8 * group : SHARED + 8 * group + 8]
        out[t] = pack_tp(share[MAIN * t : MAIN * (t + 1)], shared, (FREE - PIECE * q) % LANES)


def eleven_bits(value):
    moved = value * 8193.0
    return moved - (moved - value)


def total_kernel(arrived, gram, out):
    at = position()
    total = arrived[0]
    for t in range(1, TPS):
        total += arrived[t]
    gram[...] = total
    most = jnp.max(jnp.abs(total), keepdims=True)
    scale, factors = jnp.ones((1, 1), f32), []
    for power in (-12, *(14,) * 8, 7, 4, 2, 1):
        up = 2.0**power
        take = most >= 2.0**15 if power < 0 else most < 2.0 ** (15 - power)
        most = jnp.where(take, most * up, most)
        scale = jnp.where(take, scale * up, scale)
        factors.append(jnp.where(take, 1.0 / up, 1.0))
    total = total * scale
    high = eleven_bits(total)
    rest = total - high
    piece = pltpu.roll(rest[32:40], LANES - at[3], 1)
    parts = (rest[:48], unfolded(rest), jnp.where(lanes_of(8) // PIECE == at[5], piece, 0.0))
    left = sum(
        jnp.sum(jnp.where(eye_of(at, first, p.shape[0], at[2]), p, 0.0), axis=0, keepdims=True)
        for first, p in zip((0, 48, MAIN), parts)
    )
    left = jnp.broadcast_to(eleven_bits(left), (8, LANES))
    row, lane = rows_of(8), lanes_of(8)
    tail = jnp.where(
        row == 0, pltpu.roll(left, FREE, 1), jnp.where(row == 1, pltpu.roll(left, FREE - 32, 1), pltpu.roll(left, FREE - 64, 1))
    )
    for i, factor in enumerate(factors):
        tail = jnp.where((row == 7) & (lane == FREE + i), factor, tail)
    tail = jnp.where((row == 7) & (lane >= FREE + len(factors)), 1.0, tail)
    out[:40] = high[:40]
    out[40:] = jnp.where(lane < FREE, high[40:], tail)


def square_kernel(gram, cols, out, whole):
    at = position()
    lane = lanes_of(8)
    left = jnp.zeros((8, LANES), f32)
    inverses = []
    for t in range(TPS):
        tail = cols[t, 40:48]
        product = tail
        for shift in (1, 2, 4, 8):
            product = product * pltpu.roll(product, LANES - shift, 1)
        inverses.append(product[7:8, FREE : FREE + 1])
        left += tail * inverses[t]
    unpack_columns(cols, whole, scales=inverses)
    left = jnp.where(
        lane[:1] < 32,
        pltpu.roll(left, 32, 1)[0:1],
        jnp.where(lane[:1] < 64, pltpu.roll(left, 64, 1)[1:2], pltpu.roll(left, 96, 1)[2:3]),
    )
    own = pl.ds(pl.multiple_of(at[4], LANES), LANES)
    eye = (rows_of(LANES) == lanes_of(LANES)) & (rows_of(LANES) < COLS)
    mine = whole[own, :] + jnp.where(eye, left, 0.0)
    whole[own, :] = mine
    trace = jnp.sum(jnp.where(eye, mine, 0.0), keepdims=True)
    square = jnp.zeros((LANES, LANES), f32)
    for block in range(BLOCKS):
        value = whole[block * LANES : (block + 1) * LANES, :]
        square += value * value
    square = jnp.sum(jnp.where(lanes_of(LANES) < COLS, square, 0.0), keepdims=True)
    shared = at[1] + MAIN
    start = (shared // COLS) * LANES + shared % COLS
    shared = whole[pl.ds(pl.multiple_of(start, 8), 8), :]
    value = jnp.concatenate([gram[:48], unfolded(gram), shared], axis=0)
    row = rows_of(8)
    tail = jnp.where((row == 0) & (lane == COLS), square, jnp.where((row == 0) & (lane == COLS + 1), trace, 0.0))
    copies(out, pack_z(value, tail))


def first_kernel(rows, whole, out, poly_rows, current_rows, spectral_out, right):
    at = position()
    tails = jnp.zeros((WIDE - SPARE, LANES), f32)
    for core in range(2):
        for z in range(DEPTH):
            tails += rows[core, z, SPARE:WIDE]
    spot = rows_of(WIDE - SPARE) == 0
    lane = lanes_of(WIDE - SPARE)
    square = jnp.sum(jnp.where(spot & (lane == COLS), tails, 0.0), keepdims=True)
    trace = jnp.sum(jnp.where(spot & (lane == COLS + 1), tails, 0.0), keepdims=True)
    spectral = 2.0 * square / (trace + EPS)
    inverse = 1.0 / spectral
    spectral_out[...] = jnp.broadcast_to(spectral, spectral_out.shape)
    for block in range(BLOCKS):
        part = pl.ds(block * LANES, LANES)
        right[part, :] = (-0.5 * (whole[part, :] * inverse)).astype(bf16)
    own = pl.ds(pl.multiple_of(at[4], LANES), LANES)
    eye = (rows_of(LANES) == lanes_of(LANES)) & (rows_of(LANES) < COLS)
    right[own, :] = poly(eye, whole[own, :] * inverse).astype(bf16)

    def of_rows(part, first, col, packed):
        current = part * inverse
        return (
            poly(eye_of(at, first, part.shape[0], col), current).astype(bf16),
            current.astype(bf16),
        )

    unpack_rows(rows, at, (poly_rows, current_rows), of_rows)
    send_tp(at, out, dot(poly_rows[...], right[...]))


def next_poly(at, current):
    eye = own_eye(at)
    return poly(eye, current), jnp.sum(jnp.where(eye, current, 0.0), axis=0, keepdims=True)


def second_kernel(current_rows, cols, out_cols, out_rows, right):
    at = position()
    unpack_columns(cols, right)
    value, diag = next_poly(at, dot(current_rows[...], right[...]))
    send_tp(at, out_cols, value)
    copies(out_rows, pack_z(value, spread(diag)))


def third_kernel(poly_rows, rows, cols, out, right, kept, rows_kept, first_rows, current_rows):
    at = position()
    unpack_columns(cols, right)
    diagonal = [jnp.zeros((count, LANES), f32) for count in (WIDE, 8, 8)]

    def of_rows(part, first, col, packed):
        eye = eye_of(at, first, part.shape[0], col)
        i = (0, WIDE, MAIN).index(first)
        part = part.astype(f32)
        row = gathered(packed)
        diagonal[i] += jnp.where(eye, row, 0.0)
        return part.astype(bf16), jnp.where(eye, row, -2.0 * part).astype(bf16)

    unpack_rows(rows, at, (first_rows, current_rows), of_rows)
    own = pl.ds(pl.multiple_of(at[4], LANES), LANES)
    product = dot(poly_rows[...], right[...])
    moved = dot(current_rows[...], right[...])
    moved_low = moved.astype(bf16).astype(f32)
    square = dot(first_rows[...], right[...])
    moved_off = moved - moved_low
    kept[0] = first_rows[:, own].astype(f32)
    kept[1] = current_rows[:, own].astype(f32)
    kept[2] = moved_off
    kept[3] = square.astype(bf16).astype(f32) - square
    kept[4] = jnp.broadcast_to(
        jnp.sum(jnp.concatenate(diagonal, axis=0), axis=1, keepdims=True), (ROWS, LANES)
    )
    eye = own_eye(at)
    tail = spread(jnp.sum(jnp.where(eye, moved_off, 0.0), axis=0, keepdims=True))
    product, moved_low = pack_z(product).astype(bf16), pack_z(moved_low, tail).astype(bf16)
    for z in range(DEPTH):
        out[z, :WIDE] = product
        out[z, WIDE:] = moved_low
    mine = right[own, :].astype(f32)
    total = jnp.zeros((LANES, LANES), f32)
    for block in range(BLOCKS):
        value = right[block * LANES : (block + 1) * LANES, :].astype(f32)
        total += value * value
    total = jnp.sum(total, axis=0, keepdims=True)
    on = rows_of(LANES) == lanes_of(LANES)
    row = rows_of(8)
    rows_kept[...] = jnp.where(
        row == 0,
        jnp.sum(jnp.where(on, mine, 0.0), axis=0, keepdims=True),
        total.astype(bf16).astype(f32) - total,
    )


def fourth_kernel(rows, right, kept, rows_kept, out, product_rows, moved_rows):
    at = position()
    diagonal = [jnp.zeros((count, LANES), f32) for count in (WIDE, 8, 8)]

    def of_rows(part, first, col, packed):
        eye = eye_of(at, first, part.shape[0], col)
        diagonal[(0, WIDE, MAIN).index(first)] += jnp.where(eye, gathered(packed), 0.0)
        return (part.astype(bf16),)

    unpack_rows(rows.at[:, :, WIDE:], at, (moved_rows,), of_rows)
    unpack_rows(rows.at[:, :, :WIDE], at, (product_rows,), lambda part, first, col, packed: (part.astype(bf16),))
    moved_diagonal = jnp.sum(jnp.concatenate(diagonal, axis=0), axis=1, keepdims=True)
    poly_own, current_own, moved_off, square_off, current_diagonal = (kept[i] for i in range(5))
    poly_diagonal, square_diagonal = rows_kept[0:1], rows_kept[1:2]
    eye = own_eye(at)
    off = jnp.where(
        eye,
        moved_off * poly_own + current_own * square_off,
        moved_diagonal * poly_own
        + moved_off * poly_diagonal
        + current_diagonal * square_off
        + current_own * square_diagonal,
    )
    send_tp(at, out, poly(eye, dot(moved_rows[...], right[...]) + off))


def fifth_kernel(product_rows, cols, out, right):
    at = position()
    unpack_columns(cols, right)
    send_tp(at, out, dot(product_rows[...], right[...]))


def last_kernel(cols, whole0, whole1, spectral, out_gate, out_up, product):
    for t in range(TPS):
        packed = cols[t]
        product[MAIN * t : MAIN * t + 48, :] = packed
        product[MAIN * t + 48 : MAIN * (t + 1), :] = unfolded(packed).astype(bf16)
    lane = lanes_of(8)
    for group in range(TPS // 4):
        value = pltpu.roll(cols[4 * group + 3, 32:40].astype(f32), PIECE * 3 + LANES - FREE, 1)
        for q in (2, 1, 0):
            part = pltpu.roll(cols[4 * group + q, 32:40].astype(f32), PIECE * q + LANES - FREE, 1)
            value = jnp.where(lane < PIECE * (q + 1), part, value)
        product[SHARED + 8 * group : SHARED + 8 * (group + 1), :] = value.astype(bf16)
    half = D // 2
    ortho = sum(
        lax.dot_general(
            product[h * half : (h + 1) * half, :],
            whole[...],
            (((0,), (0,)), ((), ())),
            preferred_element_type=f32,
        )
        for h, whole in enumerate((whole0, whole1))
    )
    ortho = ortho[:COLS] * jnp.sqrt(2.0 * FF / spectral[0:1, 0:1])
    width = out_gate.shape[1]
    out_gate[...] = ortho[:, :width]
    out_up[...] = ortho[:, width : 2 * width]


def call(kernel, outs, *args, scratch=()):
    vmem = pl.BlockSpec(memory_space=pltpu.VMEM)
    return pl.pallas_call(
        kernel,
        out_shape=[jax.ShapeDtypeStruct(shape, dtype) for shape, dtype in outs],
        in_specs=[vmem] * len(args),
        out_specs=[vmem] * len(outs),
        scratch_shapes=[pltpu.VMEM(shape, dtype) for shape, dtype in scratch],
        compiler_params=pltpu.CompilerParams(vmem_limit_bytes=24 * 2**20),
        name=kernel.__name__,
    )(*args)


def exchange(stacked, axes):
    return lax.all_to_all(stacked, axes, split_axis=0, concat_axis=0, tiled=True)


def both_cores(by_z):
    return lax.all_gather(by_z, "core")


def local(grad_gate, grad_up, moment_gate, moment_up):
    gate_next = BETA * moment_gate + grad_gate
    up_next = BETA * moment_up + grad_up
    half = gate_next.shape[1]
    low = jnp.concatenate([gate_next.astype(bf16), up_next.astype(bf16)], axis=1)
    low = jnp.pad(low, ((0, 0), (0, 3 * LANES - 2 * half)))
    by_z = lax.all_gather(low, "z")
    whole = [
        lax.all_gather(by_z[h * NEAR : (h + 1) * NEAR], "core").reshape(D // 2, -1) for h in range(2)
    ]

    right = ((KDIM, LANES), bf16)
    left = ((ROWS, KDIM), bf16)
    block = ((ROWS, LANES), f32)
    to_tp, to_z = ((TPS, SENT, LANES), bf16), ((DEPTH, WIDE, LANES), bf16)
    to_tp32, to_z32 = (to_tp[0], f32), (to_z[0], f32)

    (shares,) = call(
        gram_kernel, [to_tp32], low, *whole, scratch=[((LANES, low.shape[1]), bf16), ((D, LANES), f32)]
    )
    gram, sent = call(total_kernel, [((SENT, LANES), f32)] * 2, exchange(shares, TP))
    sent = jnp.broadcast_to(sent.astype(jnp.float16), to_tp[0])
    cols = exchange(sent, TP).astype(f32)
    rows, gram_cols = call(square_kernel, [to_z32, (right[0], f32)], gram, cols)
    rows = both_cores(exchange(rows, "z"))
    sent, poly_rows, current_rows, spectral = call(
        first_kernel, [to_tp, left, left, ((8, LANES), f32)], rows, gram_cols, scratch=[right]
    )
    cols, rows = call(second_kernel, [to_tp, to_z], current_rows, exchange(sent, TP), scratch=[right])
    rows = both_cores(exchange(rows, "z"))
    cols = exchange(cols, TP)
    rows, right_poly, kept, rows_kept = call(
        third_kernel,
        [((DEPTH, 2 * WIDE, LANES), bf16), right, ((5, ROWS, LANES), f32), ((8, LANES), f32)],
        poly_rows,
        rows,
        cols,
        scratch=[left, left],
    )
    rows = both_cores(exchange(rows, "z"))
    cols, product_rows = call(
        fourth_kernel, [to_tp, left], rows, right_poly, kept, rows_kept, scratch=[left]
    )
    (cols,) = call(fifth_kernel, [to_tp], product_rows, exchange(cols, TP), scratch=[right])
    ortho_gate, ortho_up = call(
        last_kernel,
        [((COLS, half), f32)] * 2,
        exchange(cols, TP),
        *whole,
        spectral,
        scratch=[((D, LANES), bf16)],
    )
    return gate_next, up_next, ortho_gate, ortho_up


def solution(mesh):
    split = Mesh(mesh.devices.reshape(DEPTH, 2, 8, 4), ("z", "core", "y", "x"))
    spec = P(FS, TP)
    return jax.shard_map(
        local, mesh=split, in_specs=(spec,) * 4, out_specs=(spec,) * 4, check_vma=False
    )
```

```python
import jax
import jax.numpy as jnp
from jax import lax
from jax.experimental import pallas as pl
from jax.experimental.pallas import tpu as pltpu
from jax.sharding import Mesh
from jax.sharding import PartitionSpec as P

FF = 5632
FS = ("z", "core")
TP = ("y", "x")
BETA = 0.95
EPS = 1e-06
LANES = 128
D = 2112
COLS = 88
BLOCKS = D // COLS
DEPTH = 12
NEAR = 6
TPS = 32
MAIN = 64
SHARED = TPS * MAIN
ROWS = MAIN + 8
PIECE = COLS // 4
SENT = 48
WIDE = 56
FREE = 96
SPARE = 48
KDIM = BLOCKS * LANES
f32, bf16, f16 = jnp.float32, jnp.bfloat16, jnp.float16


def place(core, z):
    return ((z // NEAR) * 2 + core) * NEAR + z % NEAR


def lanes_of(rows):
    return lax.broadcasted_iota(jnp.int32, (rows, LANES), 1)


def rows_of(rows):
    return lax.broadcasted_iota(jnp.int32, (rows, LANES), 0)


def folded(block, low):
    lane = lanes_of(16)
    return [
        jnp.where(lane < COLS, block[16 * i : 16 * i + 16], pltpu.roll(low, shift, 1))
        for i, shift in enumerate((COLS, COLS - 40, COLS - 80))
    ]


def unfolded(packed):
    lane = lanes_of(16)
    a, b, c = (
        pltpu.roll(packed[16 * i : 16 * i + 16].astype(f32), shift, 1)
        for i, shift in enumerate((40, 80, 120))
    )
    return jnp.where(lane < 40, a, jnp.where(lane < 80, b, c))


def pack_tp(main, shared, shift, tail=None):
    a, b, c = folded(main, main[48:64])
    top = jnp.where(lanes_of(8) < FREE, c[:8], pltpu.roll(shared, shift, 1))
    end = c[8:] if tail is None else jnp.where(lanes_of(8) < FREE, c[8:], tail)
    return jnp.concatenate([a, b, top, end], axis=0)


def pack_z(block, tail=None):
    end = block[SPARE:WIDE]
    if tail is not None:
        end = jnp.where(lanes_of(WIDE - SPARE) < COLS, end, tail)
    return jnp.concatenate([*folded(block, block[WIDE:ROWS]), end], axis=0)


def spread(row):
    row = jnp.broadcast_to(row, (WIDE - SPARE, LANES))
    at = rows_of(WIDE - SPARE)
    return jnp.where(
        at == 0,
        pltpu.roll(row, COLS, 1),
        jnp.where(at == 1, pltpu.roll(row, COLS - 40, 1), pltpu.roll(row, COLS - 80, 1)),
    )


def gathered(packed):
    tail = packed[SPARE:WIDE].astype(f32)
    lane = lanes_of(1)
    return jnp.where(
        lane < 40,
        pltpu.roll(tail, 40, 1)[0:1],
        jnp.where(lane < 80, pltpu.roll(tail, 80, 1)[1:2], pltpu.roll(tail, 120, 1)[2:3]),
    )


def store_rows(target, first, value):
    at, last = first, first + value.shape[0]
    while at < last:
        block, row = divmod(at, COLS)
        count = min(COLS - row, last - at)
        start = block * LANES + row
        target[start : start + count, :] = value[at - first : at - first + count].astype(target.dtype)
        at += count


def unpack_columns(blocks, target, scales=None):
    def scaled(part, t):
        return part if scales is None else part * scales[t]

    for block in range(BLOCKS):
        target[block * LANES + COLS : (block + 1) * LANES, :] = jnp.zeros((LANES - COLS, LANES), target.dtype)
    for t in range(TPS):
        packed = blocks[t]
        store_rows(target, MAIN * t, scaled(packed, t))
        store_rows(target, MAIN * t + 48, scaled(unfolded(packed), t))
    lane = lanes_of(8)
    for group in range(TPS // 4):
        parts = [
            scaled(
                pltpu.roll(blocks[4 * group + q, 32:40].astype(f32), PIECE * q + LANES - FREE, 1), 4 * group + q
            )
            for q in range(4)
        ]
        value = parts[3]
        for q in (2, 1, 0):
            value = jnp.where(lane < PIECE * (q + 1), parts[q], value)
        store_rows(target, SHARED + 8 * group, value)


def unpack_rows(blocks, at, targets, change):
    for core in range(2):
        for z in range(DEPTH):
            b = place(core, z)
            packed = blocks[core, z]
            low = unfolded(packed)
            for first, part in ((0, packed), (WIDE, low[:8]), (MAIN, low[8:])):
                for target, value in zip(targets, change(part, first, b * COLS, packed)):
                    target[first : first + part.shape[0], b * LANES : (b + 1) * LANES] = value


def position():
    own = place(lax.axis_index("core"), lax.axis_index("z"))
    t = lax.axis_index("y") * 4 + lax.axis_index("x")
    return (
        t * MAIN,
        SHARED + 8 * (t // 4) - MAIN,
        own * COLS,
        (FREE + LANES - PIECE * (t % 4)) % LANES,
        own * LANES,
        t % 4,
    )


def eye_of(at, first, count, col):
    row = at[0] if first < MAIN else at[1]
    return (rows_of(count) + (row + first) == lanes_of(count) + col) & (lanes_of(count) < COLS)


def own_eye(at):
    return jnp.concatenate([eye_of(at, 0, MAIN, at[2]), eye_of(at, MAIN, ROWS - MAIN, at[2])], axis=0)


def poly(eye, current):
    return jnp.where(eye, 1.5 - 0.5 * current, -0.5 * current)


def dot(left, right):
    return jnp.dot(left, right, preferred_element_type=f32)


def copies(out, value):
    value = value.astype(out.dtype)
    for i in range(out.shape[0]):
        out[i] = value


def send_tp(at, out, block, tail=None):
    copies(out, pack_tp(block[:MAIN], block[MAIN:ROWS], at[3], tail))


def eleven_bits(value):
    moved = value * 8193.0
    return moved - (moved - value)


def float16_scale(most):
    scale, factors = jnp.ones((1, 1), f32), []
    for power in (*(-14,) * 5, *(14,) * 8, 7, 4, 2, 1):
        up = 2.0**power
        take = most >= 2.0**15 if power < 0 else most < 2.0 ** (15 - power)
        most = jnp.where(take, most * up, most)
        scale = jnp.where(take, scale * up, scale)
        factors.append(jnp.where(take, 1.0 / up, 1.0))
    return scale, factors


FACTORS = 17
WORDS = 32


def with_row(tail, at, lane, values):
    row, lanes = rows_of(8), lanes_of(8)
    for i, value in enumerate(values):
        tail = jnp.where((row == at) & (lanes == lane + i), value, tail)
    return tail


def with_factors(tail, at, lane, factors):
    row, lanes = rows_of(8), lanes_of(8)
    tail = jnp.where((row == at) & (lanes >= lane) & (lanes < lane + WORDS), 1.0, tail)
    return with_row(tail, at, lane, factors)


def products(tail):
    for shift in (1, 2, 4, 8, 16):
        tail = tail * pltpu.roll(tail, LANES - shift, 1)
    return tail


def tail_tp(left, factors):
    left, row = jnp.broadcast_to(left, (8, LANES)), rows_of(8)
    tail = jnp.where(
        row == 0,
        pltpu.roll(left, FREE, 1),
        jnp.where(row == 1, pltpu.roll(left, FREE - 32, 1), pltpu.roll(left, FREE - 64, 1)),
    )
    return with_factors(tail, 7, FREE, factors)


def left_tp(tail):
    lane = lanes_of(1)
    return jnp.where(
        lane < 32,
        pltpu.roll(tail, 32, 1)[0:1],
        jnp.where(lane < 64, pltpu.roll(tail, 64, 1)[1:2], pltpu.roll(tail, 96, 1)[2:3]),
    )


def own_square():
    return (rows_of(LANES) == lanes_of(LANES)) & (rows_of(LANES) < COLS)


def gram_kernel(low, whole0, whole1, out, own, share):
    at = position()
    own[:COLS] = low[...]
    own[COLS:] = jnp.zeros((LANES - COLS, own.shape[1]), bf16)
    half = D // 2
    most = jnp.zeros((1, 1), f32)
    for h, whole in enumerate((whole0, whole1)):
        part = lax.dot_general(
            whole[...], own[...], (((1,), (1,)), ((), ())), preferred_element_type=f32
        )
        share[h * half : (h + 1) * half] = part
        most = jnp.maximum(most, jnp.max(jnp.abs(part), keepdims=True))
    scale, factors = float16_scale(most)
    mine = share[pl.ds(pl.multiple_of(at[2], 8), COLS), :] * scale
    eye = rows_of(COLS) == lanes_of(COLS)
    left = jnp.sum(jnp.where(eye, mine - eleven_bits(mine), 0.0), axis=0, keepdims=True)
    tail = tail_tp(eleven_bits(left), factors)
    for t in range(TPS):
        group, q = divmod(t, 4)
        main = eleven_bits(share[MAIN * t : MAIN * (t + 1)] * scale)
        shared = eleven_bits(share[SHARED + 8 * group : SHARED + 8 * group + 8] * scale)
        out[t] = pack_tp(main, shared, (FREE - PIECE * q) % LANES, tail)


def total_kernel(arrived, gram, out):
    at = position()
    total, left = jnp.zeros((SENT, LANES), f32), jnp.zeros((8, LANES), f32)
    for t in range(TPS):
        tail = arrived[t, 40:]
        inverse = products(tail)[7:8, FREE : FREE + 1]
        total += arrived[t] * inverse
        left += tail * inverse
    piece = pltpu.roll(total[32:40], LANES - at[3], 1)
    piece = jnp.where(lanes_of(8) // PIECE == at[5], piece, 0.0)
    total = jnp.concatenate([total[:48], unfolded(total), piece], axis=0)
    total = jnp.where(lanes_of(ROWS) < COLS, total, 0.0)
    eye = own_eye(at) & ((rows_of(ROWS) < MAIN) | (lanes_of(ROWS) // PIECE == at[5]))
    total += jnp.where(eye, left_tp(left), 0.0)
    gram[...] = total
    scale, factors = float16_scale(jnp.max(jnp.abs(total), keepdims=True))
    total = total * scale
    high = eleven_bits(total)
    left = jnp.sum(jnp.where(eye, total - high, 0.0), axis=0, keepdims=True)
    out[...] = pack_tp(high[:MAIN], high[MAIN:], at[3], tail_tp(eleven_bits(left), factors))


def square_kernel(gram, cols, out, whole):
    at = position()
    left = jnp.zeros((8, LANES), f32)
    inverses = []
    for t in range(TPS):
        tail = cols[t, 40:]
        inverses.append(products(tail)[7:8, FREE : FREE + 1])
        left += tail * inverses[t]
    unpack_columns(cols, whole, scales=inverses)
    own = pl.ds(pl.multiple_of(at[4], LANES), LANES)
    mine = whole[own, :] + jnp.where(own_square(), left_tp(left), 0.0)
    whole[own, :] = mine
    trace = jnp.sum(jnp.where(own_square(), mine, 0.0), keepdims=True)
    square = jnp.zeros((LANES, LANES), f32)
    for block in range(BLOCKS):
        value = whole[block * LANES : (block + 1) * LANES, :]
        square += value * value
    square = jnp.sum(jnp.where(lanes_of(LANES) < COLS, square, 0.0), keepdims=True)
    shared = at[1] + MAIN
    start = (shared // COLS) * LANES + shared % COLS
    shared = whole[pl.ds(pl.multiple_of(start, 8), 8), :]
    value = jnp.concatenate([gram[:MAIN], jnp.where(lanes_of(8) < COLS, shared, 0.0)], axis=0)
    scale, factors = float16_scale(jnp.max(jnp.abs(value), keepdims=True))
    value = value * scale
    high = eleven_bits(value)
    left = jnp.sum(jnp.where(own_eye(at), value - high, 0.0), axis=0, keepdims=True)
    tail = with_factors(spread(eleven_bits(left)), 3, COLS, factors)
    for i, number in enumerate((square, trace)):
        scale, factors = float16_scale(number)
        rest, words = number * scale, []
        for _ in range(3):
            words.append(eleven_bits(rest))
            rest = rest - words[-1]
        tail = with_row(with_factors(tail, 4 + i, COLS, factors), 4 + i, COLS + WORDS, words)
    out[...] = pack_z(high, tail)


def first_kernel(rows, whole, out, poly_rows, current_rows, spectral_out, right):
    at = position()
    inverses = {}
    square, trace = jnp.zeros((1, 1), f32), jnp.zeros((1, 1), f32)
    for core in range(2):
        for z in range(DEPTH):
            tail = rows[core, z, SPARE:WIDE]
            factor = products(tail)[:, COLS : COLS + 1]
            word = (tail[:, COLS + WORDS + 2 : COLS + WORDS + 3] + tail[:, COLS + WORDS + 1 : COLS + WORDS + 2]) + tail[
                :, COLS + WORDS : COLS + WORDS + 1
            ]
            inverses[place(core, z)] = factor[3:4]
            square += word[4:5] * factor[4:5]
            trace += word[5:6] * factor[5:6]
    spectral = 2.0 * square / (trace + EPS)
    inverse = 1.0 / spectral
    spectral_out[...] = jnp.broadcast_to(spectral, spectral_out.shape)
    for block in range(BLOCKS):
        part = pl.ds(block * LANES, LANES)
        right[part, :] = (-0.5 * (whole[part, :] * inverse)).astype(bf16)
    own = pl.ds(pl.multiple_of(at[4], LANES), LANES)
    right[own, :] = poly(own_square(), whole[own, :] * inverse).astype(bf16)

    def of_rows(part, first, col, packed):
        eye = eye_of(at, first, part.shape[0], col)
        whole_part = jnp.where(eye, part + gathered(packed), part) * inverses[col // COLS]
        current = whole_part * inverse
        return poly(eye, current).astype(bf16), current.astype(bf16)

    unpack_rows(rows, at, (poly_rows, current_rows), of_rows)
    send_tp(at, out, dot(poly_rows[...], right[...]))


def next_poly(at, current):
    eye = own_eye(at)
    return poly(eye, current), jnp.sum(jnp.where(eye, current, 0.0), axis=0, keepdims=True)


def second_kernel(current_rows, cols, out_cols, out_rows, right):
    at = position()
    unpack_columns(cols, right)
    value, diag = next_poly(at, dot(current_rows[...], right[...]))
    send_tp(at, out_cols, value)
    copies(out_rows, pack_z(value, spread(diag)))


def third_kernel(poly_rows, rows, cols, out, right, kept, rows_kept, first_rows, current_rows):
    at = position()
    unpack_columns(cols, right)
    diagonal = [jnp.zeros((count, LANES), f32) for count in (WIDE, 8, 8)]

    def of_rows(part, first, col, packed):
        eye = eye_of(at, first, part.shape[0], col)
        i = (0, WIDE, MAIN).index(first)
        part = part.astype(f32)
        row = gathered(packed)
        diagonal[i] += jnp.where(eye, row, 0.0)
        return part.astype(bf16), jnp.where(eye, row, -2.0 * part).astype(bf16)

    unpack_rows(rows, at, (first_rows, current_rows), of_rows)
    own = pl.ds(pl.multiple_of(at[4], LANES), LANES)
    product = dot(poly_rows[...], right[...])
    moved = dot(current_rows[...], right[...])
    moved_low = moved.astype(bf16).astype(f32)
    square = dot(first_rows[...], right[...])
    moved_off = moved - moved_low
    kept[0] = first_rows[:, own].astype(f32)
    kept[1] = current_rows[:, own].astype(f32)
    kept[2] = moved_off
    kept[3] = square.astype(bf16).astype(f32) - square
    kept[4] = jnp.broadcast_to(
        jnp.sum(jnp.concatenate(diagonal, axis=0), axis=1, keepdims=True), (ROWS, LANES)
    )
    eye = own_eye(at)
    tail = spread(jnp.sum(jnp.where(eye, moved_off, 0.0), axis=0, keepdims=True))
    product, moved_low = pack_z(product).astype(bf16), pack_z(moved_low, tail).astype(bf16)
    for z in range(DEPTH):
        out[z, :WIDE] = product
        out[z, WIDE:] = moved_low
    mine = right[own, :].astype(f32)
    total = jnp.zeros((LANES, LANES), f32)
    for block in range(BLOCKS):
        value = right[block * LANES : (block + 1) * LANES, :].astype(f32)
        total += value * value
    total = jnp.sum(total, axis=0, keepdims=True)
    on = rows_of(LANES) == lanes_of(LANES)
    row = rows_of(8)
    rows_kept[...] = jnp.where(
        row == 0,
        jnp.sum(jnp.where(on, mine, 0.0), axis=0, keepdims=True),
        total.astype(bf16).astype(f32) - total,
    )


def fourth_kernel(rows, right, kept, rows_kept, out, product_rows, moved_rows):
    at = position()
    diagonal = [jnp.zeros((count, LANES), f32) for count in (WIDE, 8, 8)]

    def of_rows(part, first, col, packed):
        eye = eye_of(at, first, part.shape[0], col)
        diagonal[(0, WIDE, MAIN).index(first)] += jnp.where(eye, gathered(packed), 0.0)
        return (part.astype(bf16),)

    unpack_rows(rows.at[:, :, WIDE:], at, (moved_rows,), of_rows)
    unpack_rows(rows.at[:, :, :WIDE], at, (product_rows,), lambda part, first, col, packed: (part.astype(bf16),))
    moved_diagonal = jnp.sum(jnp.concatenate(diagonal, axis=0), axis=1, keepdims=True)
    poly_own, current_own, moved_off, square_off, current_diagonal = (kept[i] for i in range(5))
    poly_diagonal, square_diagonal = rows_kept[0:1], rows_kept[1:2]
    eye = own_eye(at)
    off = jnp.where(
        eye,
        moved_off * poly_own + current_own * square_off,
        moved_diagonal * poly_own
        + moved_off * poly_diagonal
        + current_diagonal * square_off
        + current_own * square_diagonal,
    )
    send_tp(at, out, poly(eye, dot(moved_rows[...], right[...]) + off))


def fifth_kernel(product_rows, cols, out, right):
    at = position()
    unpack_columns(cols, right)
    send_tp(at, out, dot(product_rows[...], right[...]))


def last_kernel(cols, whole0, whole1, spectral, out_gate, out_up, product):
    for t in range(TPS):
        packed = cols[t]
        product[MAIN * t : MAIN * t + 48, :] = packed
        product[MAIN * t + 48 : MAIN * (t + 1), :] = unfolded(packed).astype(bf16)
    lane = lanes_of(8)
    for group in range(TPS // 4):
        value = pltpu.roll(cols[4 * group + 3, 32:40].astype(f32), PIECE * 3 + LANES - FREE, 1)
        for q in (2, 1, 0):
            part = pltpu.roll(cols[4 * group + q, 32:40].astype(f32), PIECE * q + LANES - FREE, 1)
            value = jnp.where(lane < PIECE * (q + 1), part, value)
        product[SHARED + 8 * group : SHARED + 8 * (group + 1), :] = value.astype(bf16)
    half = D // 2
    ortho = sum(
        lax.dot_general(
            product[h * half : (h + 1) * half, :],
            whole[...],
            (((0,), (0,)), ((), ())),
            preferred_element_type=f32,
        )
        for h, whole in enumerate((whole0, whole1))
    )
    ortho = ortho[:COLS] * jnp.sqrt(2.0 * FF / spectral[0:1, 0:1])
    width = out_gate.shape[1]
    out_gate[...] = ortho[:, :width]
    out_up[...] = ortho[:, width : 2 * width]


def call(kernel, outs, *args, scratch=()):
    vmem = pl.BlockSpec(memory_space=pltpu.VMEM)
    return pl.pallas_call(
        kernel,
        out_shape=[jax.ShapeDtypeStruct(shape, dtype) for shape, dtype in outs],
        in_specs=[vmem] * len(args),
        out_specs=[vmem] * len(outs),
        scratch_shapes=[pltpu.VMEM(shape, dtype) for shape, dtype in scratch],
        compiler_params=pltpu.CompilerParams(vmem_limit_bytes=24 * 2**20),
        name=kernel.__name__,
    )(*args)


def exchange(stacked, axes):
    return lax.all_to_all(stacked, axes, split_axis=0, concat_axis=0, tiled=True)


def both_cores(by_z):
    return lax.all_gather(by_z, "core")


def local(grad_gate, grad_up, moment_gate, moment_up):
    gate_next = BETA * moment_gate + grad_gate
    up_next = BETA * moment_up + grad_up
    half = gate_next.shape[1]
    low = jnp.concatenate([gate_next.astype(bf16), up_next.astype(bf16)], axis=1)
    low = jnp.pad(low, ((0, 0), (0, 3 * LANES - 2 * half)))
    by_z = lax.all_gather(low, "z")
    whole = [
        lax.all_gather(by_z[h * NEAR : (h + 1) * NEAR], "core").reshape(D // 2, -1) for h in range(2)
    ]

    right = ((KDIM, LANES), bf16)
    left = ((ROWS, KDIM), bf16)
    block = ((ROWS, LANES), f32)
    to_tp, to_z = ((TPS, SENT, LANES), bf16), ((DEPTH, WIDE, LANES), bf16)
    to_tp32 = (to_tp[0], f32)

    (shares,) = call(
        gram_kernel, [to_tp32], low, *whole, scratch=[((LANES, low.shape[1]), bf16), ((D, LANES), f32)]
    )
    shares = exchange(shares.astype(f16), TP).astype(f32)
    gram, sent = call(total_kernel, [((ROWS, LANES), f32), ((SENT, LANES), f32)], shares)
    cols = exchange(jnp.broadcast_to(sent.astype(f16), to_tp[0]), TP).astype(f32)
    sent, gram_cols = call(square_kernel, [((WIDE, LANES), f32), (right[0], f32)], gram, cols)
    rows = exchange(jnp.broadcast_to(sent.astype(f16), to_z[0]), "z")
    rows = both_cores(rows).astype(f32)
    sent, poly_rows, current_rows, spectral = call(
        first_kernel, [to_tp, left, left, ((8, LANES), f32)], rows, gram_cols, scratch=[right]
    )
    cols, rows = call(second_kernel, [to_tp, to_z], current_rows, exchange(sent, TP), scratch=[right])
    rows = both_cores(exchange(rows, "z"))
    cols = exchange(cols, TP)
    rows, right_poly, kept, rows_kept = call(
        third_kernel,
        [((DEPTH, 2 * WIDE, LANES), bf16), right, ((5, ROWS, LANES), f32), ((8, LANES), f32)],
        poly_rows,
        rows,
        cols,
        scratch=[left, left],
    )
    rows = both_cores(exchange(rows, "z"))
    cols, product_rows = call(
        fourth_kernel, [to_tp, left], rows, right_poly, kept, rows_kept, scratch=[left]
    )
    (cols,) = call(fifth_kernel, [to_tp], product_rows, exchange(cols, TP), scratch=[right])
    ortho_gate, ortho_up = call(
        last_kernel,
        [((COLS, half), f32)] * 2,
        exchange(cols, TP),
        *whole,
        spectral,
        scratch=[((D, LANES), bf16)],
    )
    return gate_next, up_next, ortho_gate, ortho_up


def solution(mesh):
    split = Mesh(mesh.devices.reshape(DEPTH, 2, 8, 4), ("z", "core", "y", "x"))
    spec = P(FS, TP)
    return jax.shard_map(
        local, mesh=split, in_specs=(spec,) * 4, out_specs=(spec,) * 4, check_vma=False
    )
```

```python
import jax
import jax.numpy as jnp
from jax import lax
from jax.experimental import pallas as pl
from jax.experimental.pallas import tpu as pltpu
from jax.sharding import Mesh
from jax.sharding import PartitionSpec as P

FF = 5632
FS = ("z", "core")
TP = ("y", "x")
BETA = 0.95
EPS = 1e-06
LANES = 128
D = 2112
COLS = 88
BLOCKS = D // COLS
DEPTH = 12
NEAR = 6
TPS = 32
MAIN = 64
LAST = TPS * MAIN
PAIR = 2
ROWS = MAIN + 8
SENT = 48
FREE = 96
KDIM = BLOCKS * LANES
WORDS = 32
f32, bf16, f16 = jnp.float32, jnp.bfloat16, jnp.float16


def place(core, z):
    return ((z // NEAR) * 2 + core) * NEAR + z % NEAR


def lanes_of(rows):
    return lax.broadcasted_iota(jnp.int32, (rows, LANES), 1)


def rows_of(rows):
    return lax.broadcasted_iota(jnp.int32, (rows, LANES), 0)


def position():
    own = place(lax.axis_index("core"), lax.axis_index("z"))
    t = lax.axis_index("y") * 4 + lax.axis_index("x")
    return t * MAIN, LAST + PAIR * t - MAIN, own * COLS, own * LANES


def pack(block, tail=None):
    lane, low = lanes_of(16), block[48:MAIN]
    a, b, c = (
        jnp.where(lane < COLS, block[16 * i : 16 * i + 16], pltpu.roll(low, shift, 1))
        for i, shift in enumerate((COLS, COLS - 40, COLS - 80))
    )
    last, row = block[MAIN:ROWS], rows_of(8)
    pair = jnp.where(
        row < 2,
        pltpu.roll(last, FREE, 1),
        jnp.where(
            row < 4,
            pltpu.roll(pltpu.roll(last, FREE - 32, 1), 2, 0),
            pltpu.roll(pltpu.roll(last, FREE - 64, 1), 4, 0),
        ),
    )
    used = lanes_of(8) < FREE
    end = c[8:] if tail is None else jnp.where(used, c[8:], tail)
    return jnp.concatenate([a, b, jnp.where(used, c[:8], pair), end], axis=0)


def low_rows(packed):
    lane = lanes_of(16)
    a, b, c = (
        pltpu.roll(packed[16 * i : 16 * i + 16].astype(f32), shift, 1)
        for i, shift in enumerate((40, 80, 120))
    )
    return jnp.where(lane < 40, a, jnp.where(lane < 80, b, c))


def last_rows(packed):
    part, lane = packed[32:40].astype(f32), lanes_of(8)
    a = pltpu.roll(part, 32, 1)
    b = pltpu.roll(pltpu.roll(part, 64, 1), 6, 0)
    c = pltpu.roll(pltpu.roll(part, 96, 1), 4, 0)
    return jnp.where(lane < 32, a, jnp.where(lane < 64, b, c))


def parts_of(packed):
    return (0, packed), (48, low_rows(packed)), (MAIN, last_rows(packed))


def last_eight(blocks, group):
    row = rows_of(8)
    value = last_rows(blocks[4 * group])
    for q in (1, 2, 3):
        value = jnp.where(row < PAIR * q, value, pltpu.roll(last_rows(blocks[4 * group + q]), PAIR * q, 0))
    return value


def with_row(tail, at, lane, values):
    row, lanes = rows_of(8), lanes_of(8)
    for i, value in enumerate(values):
        tail = jnp.where((row == at) & (lanes == lane + i), value, tail)
    return tail


def with_factors(tail, at, factors):
    tail = jnp.where((rows_of(8) == at) & (lanes_of(8) >= FREE), 1.0, tail)
    return with_row(tail, at, FREE, factors)


def products(tail):
    for shift in (1, 2, 4, 8, 16):
        tail = tail * pltpu.roll(tail, LANES - shift, 1)
    return tail


def tail_of(row):
    row, at = jnp.broadcast_to(row, (8, LANES)), rows_of(8)
    return jnp.where(
        at == 0,
        pltpu.roll(row, FREE, 1),
        jnp.where(at == 1, pltpu.roll(row, FREE - 32, 1), pltpu.roll(row, FREE - 64, 1)),
    )


def row_in(tail):
    lane = lanes_of(1)
    return jnp.where(
        lane < 32,
        pltpu.roll(tail, 32, 1)[0:1],
        jnp.where(lane < 64, pltpu.roll(tail, 64, 1)[1:2], pltpu.roll(tail, 96, 1)[2:3]),
    )


def eleven_bits(value):
    moved = value * 8193.0
    return moved - (moved - value)


def float16_scale(most):
    scale, factors = jnp.ones((1, 1), f32), []
    for power in (*(-14,) * 5, *(14,) * 8, 7, 4, 2, 1):
        up = 2.0**power
        take = most >= 2.0**15 if power < 0 else most < 2.0 ** (15 - power)
        most = jnp.where(take, most * up, most)
        scale = jnp.where(take, scale * up, scale)
        factors.append(jnp.where(take, 1.0 / up, 1.0))
    return scale, factors


def store_rows(target, first, value):
    at, last = first, first + value.shape[0]
    while at < last:
        block, row = divmod(at, COLS)
        count = min(COLS - row, last - at)
        start = block * LANES + row
        target[start : start + count, :] = value[at - first : at - first + count].astype(target.dtype)
        at += count


def unpack_columns(blocks, target):
    for block in range(BLOCKS):
        target[block * LANES + COLS : (block + 1) * LANES, :] = jnp.zeros((LANES - COLS, LANES), target.dtype)
    for t in range(TPS):
        packed = blocks[t]
        store_rows(target, MAIN * t, packed)
        store_rows(target, MAIN * t + 48, low_rows(packed))
    for group in range(TPS // 4):
        store_rows(target, LAST + 8 * group, last_eight(blocks, group))


def eye_of(at, first, count, col):
    row = rows_of(count)
    use = lanes_of(count) < COLS
    if first >= MAIN:
        use &= row < PAIR
    return (row + ((at[0] if first < MAIN else at[1]) + first) == lanes_of(count) + col) & use


def own_eye(at):
    return jnp.concatenate([eye_of(at, 0, MAIN, at[2]), eye_of(at, MAIN, ROWS - MAIN, at[2])], axis=0)


def own_square():
    return (rows_of(LANES) == lanes_of(LANES)) & (rows_of(LANES) < COLS)


def poly(eye, current):
    return jnp.where(eye, 1.5 - 0.5 * current, -0.5 * current)


def dot(left, right):
    return jnp.dot(left, right, preferred_element_type=f32)


def copies(out, value):
    value = value.astype(out.dtype)
    for i in range(out.shape[0]):
        out[i] = value


def each_row_block(rows):
    for core in range(2):
        for z in range(DEPTH):
            b = place(core, z)
            yield b, slice(b * LANES, (b + 1) * LANES), rows[core, z]


def gram_kernel(low, whole0, whole1, out, own, share):
    at = position()
    own[:COLS] = low[...]
    own[COLS:] = jnp.zeros((LANES - COLS, own.shape[1]), bf16)
    half = D // 2
    most = jnp.zeros((1, 1), f32)
    for h, whole in enumerate((whole0, whole1)):
        part = lax.dot_general(
            whole[...], own[...], (((1,), (1,)), ((), ())), preferred_element_type=f32
        )
        share[h * half : (h + 1) * half] = part
        most = jnp.maximum(most, jnp.max(jnp.abs(part), keepdims=True))
    scale, factors = float16_scale(most)
    mine = share[pl.ds(pl.multiple_of(at[2], 8), COLS), :] * scale
    eye = rows_of(COLS) == lanes_of(COLS)
    left = jnp.sum(jnp.where(eye, mine - eleven_bits(mine), 0.0), axis=0, keepdims=True)
    tail = with_factors(tail_of(eleven_bits(left)), 7, factors)
    for group in range(TPS // 4):
        last = eleven_bits(share[LAST + 8 * group : LAST + 8 * group + 8] * scale)
        for q in range(4):
            t = 4 * group + q
            main = eleven_bits(share[MAIN * t : MAIN * (t + 1)] * scale)
            pair = pltpu.roll(last, 8 - PAIR * q, 0) if q else last
            out[t] = pack(jnp.concatenate([main, pair], axis=0), tail)


def total_kernel(arrived, out):
    at = position()
    total, left = jnp.zeros((SENT, LANES), f32), jnp.zeros((8, LANES), f32)
    for t in range(TPS):
        tail = arrived[t, 40:]
        inverse = products(tail)[7:8, FREE : FREE + 1]
        total += arrived[t] * inverse
        left += tail * inverse
    eye = own_eye(at)
    total = jnp.concatenate([part for _, part in parts_of(total)], axis=0)
    total = jnp.where((lanes_of(ROWS) < COLS) & (rows_of(ROWS) < MAIN + PAIR), total, 0.0)
    total += jnp.where(eye, row_in(left), 0.0)
    scale, factors = float16_scale(jnp.max(jnp.abs(total), keepdims=True))
    scaled = total * scale
    high = eleven_bits(scaled)
    left = eleven_bits(jnp.sum(jnp.where(eye, scaled - high, 0.0), axis=0, keepdims=True))
    out[...] = pack(high, with_factors(tail_of(left), 7, factors))


def square_kernel(own, cols, out, whole):
    at = position()
    left = jnp.zeros((8, LANES), f32)
    for t in range(TPS):
        tail = cols[t, 40:]
        inverse = products(tail)[7:8, FREE : FREE + 1]
        left += tail * inverse
        packed = cols[t] * inverse
        store_rows(whole, MAIN * t, packed)
        store_rows(whole, MAIN * t + 48, low_rows(packed))
        if t % 4 == 0:
            last = last_rows(packed)
        else:
            last = jnp.where(rows_of(8) < PAIR * (t % 4), last, pltpu.roll(last_rows(packed), PAIR * (t % 4), 0))
        if t % 4 == 3:
            store_rows(whole, LAST + 2 * (t - 3), last)
    for block in range(BLOCKS):
        whole[block * LANES + COLS : (block + 1) * LANES, :] = jnp.zeros((LANES - COLS, LANES), f32)
    mine = pl.ds(pl.multiple_of(at[3], LANES), LANES)
    value = whole[mine, :] + jnp.where(own_square(), row_in(left), 0.0)
    whole[mine, :] = value
    trace = jnp.sum(jnp.where(own_square(), value, 0.0), keepdims=True)
    square = jnp.zeros((LANES, LANES), f32)
    for block in range(BLOCKS):
        value = whole[block * LANES : (block + 1) * LANES, :]
        square += value * value
    square = jnp.sum(jnp.where(lanes_of(LANES) < COLS, square, 0.0), keepdims=True)
    out[:40] = own[:40]
    tail = own[40:]
    for i, number in enumerate((square, trace)):
        scale, factors = float16_scale(number)
        rest, words = number * scale, []
        for _ in range(3):
            words.append(eleven_bits(rest))
            rest = rest - words[-1]
        tail = with_row(with_factors(tail, 3 + 2 * i, factors), 4 + 2 * i, FREE, words)
    out[40:] = tail


def first_kernel(rows, whole, out, poly_rows, current_rows, spectral_out, right):
    at = position()
    inverses = {}
    square, trace = jnp.zeros((1, 1), f32), jnp.zeros((1, 1), f32)
    for b, _, packed in each_row_block(rows):
        tail = packed[40:]
        factor = products(tail)[:, FREE : FREE + 1]
        word = (tail[:, FREE + 2 : FREE + 3] + tail[:, FREE + 1 : FREE + 2]) + tail[:, FREE : FREE + 1]
        inverses[b] = factor[7:8]
        square += word[4:5] * factor[3:4]
        trace += word[6:7] * factor[5:6]
    spectral = 2.0 * square / (trace + EPS)
    inverse = 1.0 / spectral
    spectral_out[...] = jnp.broadcast_to(spectral, spectral_out.shape)
    for block in range(BLOCKS):
        part = pl.ds(block * LANES, LANES)
        right[part, :] = (-0.5 * (whole[part, :] * inverse)).astype(bf16)
    mine = pl.ds(pl.multiple_of(at[3], LANES), LANES)
    right[mine, :] = poly(own_square(), whole[mine, :] * inverse).astype(bf16)
    for b, lanes, packed in each_row_block(rows):
        left = row_in(packed[40:])
        for first, part in parts_of(packed):
            eye = eye_of(at, first, part.shape[0], b * COLS)
            current = (jnp.where(eye, part + left, part) * inverses[b]) * inverse
            poly_rows[first : first + part.shape[0], lanes] = poly(eye, current).astype(bf16)
            current_rows[first : first + part.shape[0], lanes] = current.astype(bf16)
    copies(out, pack(dot(poly_rows[...], right[...])))


def second_kernel(current_rows, cols, out_cols, out_rows, right):
    at = position()
    unpack_columns(cols, right)
    current, eye = dot(current_rows[...], right[...]), own_eye(at)
    value = poly(eye, current)
    copies(out_cols, pack(value))
    diagonal = jnp.sum(jnp.where(eye, current, 0.0), axis=0, keepdims=True)
    copies(out_rows, pack(value, tail_of(diagonal)))


def third_kernel(poly_rows, rows, cols, out, right, kept, rows_kept, first_rows, current_rows):
    at = position()
    unpack_columns(cols, right)
    diagonal = [jnp.zeros((count, LANES), f32) for count in (48, 16, 8)]
    for b, lanes, packed in each_row_block(rows):
        row = row_in(packed[40:].astype(f32))
        for i, (first, part) in enumerate(parts_of(packed)):
            count = part.shape[0]
            eye, part = eye_of(at, first, count, b * COLS), part.astype(f32)
            diagonal[i] += jnp.where(eye, row, 0.0)
            first_rows[first : first + count, lanes] = part.astype(bf16)
            current_rows[first : first + count, lanes] = jnp.where(eye, row, -2.0 * part).astype(bf16)
    own = pl.ds(pl.multiple_of(at[3], LANES), LANES)
    product = dot(poly_rows[...], right[...])
    moved = dot(current_rows[...], right[...])
    moved_low = moved.astype(bf16).astype(f32)
    square = dot(first_rows[...], right[...])
    moved_off = moved - moved_low
    kept[0] = first_rows[:, own].astype(f32)
    kept[1] = current_rows[:, own].astype(f32)
    kept[2] = moved_off
    kept[3] = square.astype(bf16).astype(f32) - square
    kept[4] = jnp.broadcast_to(
        jnp.sum(jnp.concatenate(diagonal, axis=0), axis=1, keepdims=True), (ROWS, LANES)
    )
    tail = tail_of(jnp.sum(jnp.where(own_eye(at), moved_off, 0.0), axis=0, keepdims=True))
    product, moved_low = pack(product).astype(bf16), pack(moved_low, tail).astype(bf16)
    for z in range(DEPTH):
        out[z, :SENT] = product
        out[z, SENT:] = moved_low
    mine = right[own, :].astype(f32)
    total = jnp.zeros((LANES, LANES), f32)
    for block in range(BLOCKS):
        value = right[block * LANES : (block + 1) * LANES, :].astype(f32)
        total += value * value
    total = jnp.sum(total, axis=0, keepdims=True)
    on = rows_of(LANES) == lanes_of(LANES)
    rows_kept[...] = jnp.where(
        rows_of(8) == 0,
        jnp.sum(jnp.where(on, mine, 0.0), axis=0, keepdims=True),
        total.astype(bf16).astype(f32) - total,
    )


def fourth_kernel(rows, right, kept, rows_kept, out, product_rows, moved_rows):
    at = position()
    diagonal = [jnp.zeros((count, LANES), f32) for count in (48, 16, 8)]
    for b, lanes, packed in each_row_block(rows):
        moved = packed[SENT:]
        row = row_in(moved[40:].astype(f32))
        for i, (first, part) in enumerate(parts_of(moved)):
            count = part.shape[0]
            diagonal[i] += jnp.where(eye_of(at, first, count, b * COLS), row, 0.0)
            moved_rows[first : first + count, lanes] = part.astype(bf16)
        for first, part in parts_of(packed[:SENT]):
            product_rows[first : first + part.shape[0], lanes] = part.astype(bf16)
    moved_diagonal = jnp.sum(jnp.concatenate(diagonal, axis=0), axis=1, keepdims=True)
    poly_own, current_own, moved_off, square_off, current_diagonal = (kept[i] for i in range(5))
    poly_diagonal, square_diagonal = rows_kept[0:1], rows_kept[1:2]
    eye = own_eye(at)
    off = jnp.where(
        eye,
        moved_off * poly_own + current_own * square_off,
        moved_diagonal * poly_own
        + moved_off * poly_diagonal
        + current_diagonal * square_off
        + current_own * square_diagonal,
    )
    copies(out, pack(poly(eye, dot(moved_rows[...], right[...]) + off)))


def fifth_kernel(product_rows, cols, out, right):
    unpack_columns(cols, right)
    copies(out, pack(dot(product_rows[...], right[...])))


def last_kernel(cols, whole0, whole1, spectral, out_gate, out_up, product):
    for t in range(TPS):
        packed = cols[t]
        product[MAIN * t : MAIN * t + 48, :] = packed
        product[MAIN * t + 48 : MAIN * (t + 1), :] = low_rows(packed).astype(bf16)
    for group in range(TPS // 4):
        product[LAST + 8 * group : LAST + 8 * (group + 1), :] = last_eight(cols, group).astype(bf16)
    half = D // 2
    ortho = sum(
        lax.dot_general(
            product[h * half : (h + 1) * half, :],
            whole[...],
            (((0,), (0,)), ((), ())),
            preferred_element_type=f32,
        )
        for h, whole in enumerate((whole0, whole1))
    )
    ortho = ortho[:COLS] * jnp.sqrt(2.0 * FF / spectral[0:1, 0:1])
    width = out_gate.shape[1]
    out_gate[...] = ortho[:, :width]
    out_up[...] = ortho[:, width : 2 * width]


def call(kernel, outs, *args, scratch=()):
    vmem = pl.BlockSpec(memory_space=pltpu.VMEM)
    return pl.pallas_call(
        kernel,
        out_shape=[jax.ShapeDtypeStruct(shape, dtype) for shape, dtype in outs],
        in_specs=[vmem] * len(args),
        out_specs=[vmem] * len(outs),
        scratch_shapes=[pltpu.VMEM(shape, dtype) for shape, dtype in scratch],
        compiler_params=pltpu.CompilerParams(vmem_limit_bytes=24 * 2**20),
        name=kernel.__name__,
    )(*args)


def exchange(stacked, axes):
    return lax.all_to_all(stacked, axes, split_axis=0, concat_axis=0, tiled=True)


def both_cores(by_z):
    return lax.all_gather(by_z, "core")


def local(grad_gate, grad_up, moment_gate, moment_up):
    gate_next = BETA * moment_gate + grad_gate
    up_next = BETA * moment_up + grad_up
    half = gate_next.shape[1]
    low = jnp.concatenate([gate_next.astype(bf16), up_next.astype(bf16)], axis=1)
    low = jnp.pad(low, ((0, 0), (0, 3 * LANES - 2 * half)))
    by_z = lax.all_gather(low, "z")
    whole = [
        both_cores(by_z[h * NEAR : (h + 1) * NEAR]).reshape(D // 2, -1) for h in range(2)
    ]

    right, left = ((KDIM, LANES), bf16), ((ROWS, KDIM), bf16)
    to_tp, to_z = ((TPS, SENT, LANES), bf16), ((DEPTH, SENT, LANES), bf16)
    packed = ((SENT, LANES), f32)

    (shares,) = call(
        gram_kernel,
        [(to_tp[0], f32)],
        low,
        *whole,
        scratch=[((LANES, low.shape[1]), bf16), ((D, LANES), f32)],
    )
    shares = exchange(shares.astype(f16), TP).astype(f32)
    (sent,) = call(total_kernel, [packed], shares)
    cols = exchange(jnp.broadcast_to(sent.astype(f16), to_tp[0]), TP).astype(f32)
    sent, gram_cols = call(square_kernel, [packed, (right[0], f32)], sent, cols)
    rows = exchange(jnp.broadcast_to(sent.astype(f16), to_z[0]), "z")
    rows = both_cores(rows).astype(f32)
    sent, poly_rows, current_rows, spectral = call(
        first_kernel, [to_tp, left, left, ((8, LANES), f32)], rows, gram_cols, scratch=[right]
    )
    cols, rows = call(
        second_kernel, [to_tp, to_z], current_rows, exchange(sent, TP), scratch=[right]
    )
    rows = both_cores(exchange(rows, "z"))
    cols = exchange(cols, TP)
    rows, right_poly, kept, rows_kept = call(
        third_kernel,
        [((DEPTH, 2 * SENT, LANES), bf16), right, ((5, ROWS, LANES), f32), ((8, LANES), f32)],
        poly_rows,
        rows,
        cols,
        scratch=[left, left],
    )
    rows = both_cores(exchange(rows, "z"))
    cols, product_rows = call(
        fourth_kernel, [to_tp, left], rows, right_poly, kept, rows_kept, scratch=[left]
    )
    (cols,) = call(fifth_kernel, [to_tp], product_rows, exchange(cols, TP), scratch=[right])
    ortho_gate, ortho_up = call(
        last_kernel,
        [((COLS, half), f32)] * 2,
        exchange(cols, TP),
        *whole,
        spectral,
        scratch=[((D, LANES), bf16)],
    )
    return gate_next, up_next, ortho_gate, ortho_up


def solution(mesh):
    split = Mesh(mesh.devices.reshape(DEPTH, 2, 8, 4), ("z", "core", "y", "x"))
    spec = P(FS, TP)
    return jax.shard_map(
        local, mesh=split, in_specs=(spec,) * 4, out_specs=(spec,) * 4, check_vma=False
    )
```

```python
import jax
import jax.numpy as jnp
from jax import lax
from jax.experimental import pallas as pl
from jax.experimental.pallas import tpu as pltpu
from jax.sharding import Mesh
from jax.sharding import PartitionSpec as P

FF = 5632
FS = ("z", "core")
TP = ("y", "x")
BETA = 0.95
EPS = 1e-06
LANES = 128
D = 2112
COLS = 88
BLOCKS = D // COLS
DEPTH = 12
SIDE = DEPTH * 88
TPS = 32
MAIN = 64
LAST = TPS * MAIN
PAIR = 2
ROWS = MAIN + 8
SENT = 48
FREE = 96
KDIM = BLOCKS * LANES
WORDS = 32
f32, bf16, f16 = jnp.float32, jnp.bfloat16, jnp.float16


def place(core, z):
    return core * DEPTH + z


def sides():
    core = lax.axis_index("core")
    return tuple(pl.ds(pl.multiple_of(c * SIDE, 8), SIDE) for c in (core, 1 - core))


def lanes_of(rows):
    return lax.broadcasted_iota(jnp.int32, (rows, LANES), 1)


def rows_of(rows):
    return lax.broadcasted_iota(jnp.int32, (rows, LANES), 0)


def position():
    own = place(lax.axis_index("core"), lax.axis_index("z"))
    t = lax.axis_index("y") * 4 + lax.axis_index("x")
    return t * MAIN, LAST + PAIR * t - MAIN, own * COLS, own * LANES


def pack(block, tail=None):
    lane, low = lanes_of(16), block[48:MAIN]
    a, b, c = (
        jnp.where(lane < COLS, block[16 * i : 16 * i + 16], pltpu.roll(low, shift, 1))
        for i, shift in enumerate((COLS, COLS - 40, COLS - 80))
    )
    last, row = block[MAIN:ROWS], rows_of(8)
    pair = jnp.where(
        row < 2,
        pltpu.roll(last, FREE, 1),
        jnp.where(
            row < 4,
            pltpu.roll(pltpu.roll(last, FREE - 32, 1), 2, 0),
            pltpu.roll(pltpu.roll(last, FREE - 64, 1), 4, 0),
        ),
    )
    used = lanes_of(8) < FREE
    end = c[8:] if tail is None else jnp.where(used, c[8:], tail)
    return jnp.concatenate([a, b, jnp.where(used, c[:8], pair), end], axis=0)


def low_rows(packed):
    lane = lanes_of(16)
    a, b, c = (
        pltpu.roll(packed[16 * i : 16 * i + 16].astype(f32), shift, 1)
        for i, shift in enumerate((40, 80, 120))
    )
    return jnp.where(lane < 40, a, jnp.where(lane < 80, b, c))


def last_rows(packed):
    part, lane = packed[32:40].astype(f32), lanes_of(8)
    a = pltpu.roll(part, 32, 1)
    b = pltpu.roll(pltpu.roll(part, 64, 1), 6, 0)
    c = pltpu.roll(pltpu.roll(part, 96, 1), 4, 0)
    return jnp.where(lane < 32, a, jnp.where(lane < 64, b, c))


def parts_of(packed):
    return (0, packed), (48, low_rows(packed)), (MAIN, last_rows(packed))


def last_eight(blocks, group):
    row = rows_of(8)
    value = last_rows(blocks[4 * group])
    for q in (1, 2, 3):
        value = jnp.where(row < PAIR * q, value, pltpu.roll(last_rows(blocks[4 * group + q]), PAIR * q, 0))
    return value


def with_row(tail, at, lane, values):
    row, lanes = rows_of(8), lanes_of(8)
    for i, value in enumerate(values):
        tail = jnp.where((row == at) & (lanes == lane + i), value, tail)
    return tail


def with_factors(tail, at, factors):
    tail = jnp.where((rows_of(8) == at) & (lanes_of(8) >= FREE), 1.0, tail)
    return with_row(tail, at, FREE, factors)


def products(tail):
    for shift in (1, 2, 4, 8, 16):
        tail = tail * pltpu.roll(tail, LANES - shift, 1)
    return tail


def tail_of(row):
    row, at = jnp.broadcast_to(row, (8, LANES)), rows_of(8)
    return jnp.where(
        at == 0,
        pltpu.roll(row, FREE, 1),
        jnp.where(at == 1, pltpu.roll(row, FREE - 32, 1), pltpu.roll(row, FREE - 64, 1)),
    )


def row_in(tail):
    lane = lanes_of(1)
    return jnp.where(
        lane < 32,
        pltpu.roll(tail, 32, 1)[0:1],
        jnp.where(lane < 64, pltpu.roll(tail, 64, 1)[1:2], pltpu.roll(tail, 96, 1)[2:3]),
    )


def eleven_bits(value):
    moved = value * 8193.0
    return moved - (moved - value)


def float16_scale(most):
    scale, factors = jnp.ones((1, 1), f32), []
    for power in (*(-14,) * 5, *(14,) * 8, 7, 4, 2, 1):
        up = 2.0**power
        take = most >= 2.0**15 if power < 0 else most < 2.0 ** (15 - power)
        most = jnp.where(take, most * up, most)
        scale = jnp.where(take, scale * up, scale)
        factors.append(jnp.where(take, 1.0 / up, 1.0))
    return scale, factors


def store_rows(target, first, value):
    at, last = first, first + value.shape[0]
    while at < last:
        block, row = divmod(at, COLS)
        count = min(COLS - row, last - at)
        start = block * LANES + row
        target[start : start + count, :] = value[at - first : at - first + count].astype(target.dtype)
        at += count


def unpack_columns(blocks, target):
    for block in range(BLOCKS):
        target[block * LANES + COLS : (block + 1) * LANES, :] = jnp.zeros((LANES - COLS, LANES), target.dtype)
    for t in range(TPS):
        packed = blocks[t]
        store_rows(target, MAIN * t, packed)
        store_rows(target, MAIN * t + 48, low_rows(packed))
    for group in range(TPS // 4):
        store_rows(target, LAST + 8 * group, last_eight(blocks, group))


def eye_of(at, first, count, col):
    row = rows_of(count)
    use = lanes_of(count) < COLS
    if first >= MAIN:
        use &= row < PAIR
    return (row + ((at[0] if first < MAIN else at[1]) + first) == lanes_of(count) + col) & use


def own_eye(at):
    return jnp.concatenate([eye_of(at, 0, MAIN, at[2]), eye_of(at, MAIN, ROWS - MAIN, at[2])], axis=0)


def own_square():
    return (rows_of(LANES) == lanes_of(LANES)) & (rows_of(LANES) < COLS)


def poly(eye, current):
    return jnp.where(eye, 1.5 - 0.5 * current, -0.5 * current)


def dot(left, right):
    return jnp.dot(left, right, preferred_element_type=f32)


def copies(out, value):
    value = value.astype(out.dtype)
    for i in range(out.shape[0]):
        out[i] = value


def each_row_block(rows):
    for core in range(2):
        for z in range(DEPTH):
            b = place(core, z)
            yield b, slice(b * LANES, (b + 1) * LANES), rows[core, z]


def side_kernel(low, whole, out, own):
    own[:COLS] = low[...]
    own[COLS:] = jnp.zeros((LANES - COLS, own.shape[1]), bf16)
    out[...] = lax.dot_general(
        whole[...], own[...], (((1,), (1,)), ((), ())), preferred_element_type=f32
    )


def gram_kernel(low, whole, side, out, own, share):
    at = position()
    own[:COLS] = low[...]
    own[COLS:] = jnp.zeros((LANES - COLS, own.shape[1]), bf16)
    here, there = sides()
    part = side[...]
    most = jnp.max(jnp.abs(part), keepdims=True)
    share[here] = part
    part = lax.dot_general(
        whole[...], own[...], (((1,), (1,)), ((), ())), preferred_element_type=f32
    )
    most = jnp.maximum(most, jnp.max(jnp.abs(part), keepdims=True))
    share[there] = part
    scale, factors = float16_scale(most)
    mine = share[pl.ds(pl.multiple_of(at[2], 8), COLS), :] * scale
    eye = rows_of(COLS) == lanes_of(COLS)
    left = jnp.sum(jnp.where(eye, mine - eleven_bits(mine), 0.0), axis=0, keepdims=True)
    tail = with_factors(tail_of(eleven_bits(left)), 7, factors)
    for group in range(TPS // 4):
        last = eleven_bits(share[LAST + 8 * group : LAST + 8 * group + 8] * scale)
        for q in range(4):
            t = 4 * group + q
            main = eleven_bits(share[MAIN * t : MAIN * (t + 1)] * scale)
            pair = pltpu.roll(last, 8 - PAIR * q, 0) if q else last
            out[t] = pack(jnp.concatenate([main, pair], axis=0), tail)


def total_kernel(arrived, out):
    at = position()
    total, left = jnp.zeros((SENT, LANES), f32), jnp.zeros((8, LANES), f32)
    for t in range(TPS):
        tail = arrived[t, 40:]
        inverse = products(tail)[7:8, FREE : FREE + 1]
        total += arrived[t] * inverse
        left += tail * inverse
    eye = own_eye(at)
    total = jnp.concatenate([part for _, part in parts_of(total)], axis=0)
    total = jnp.where((lanes_of(ROWS) < COLS) & (rows_of(ROWS) < MAIN + PAIR), total, 0.0)
    total += jnp.where(eye, row_in(left), 0.0)
    scale, factors = float16_scale(jnp.max(jnp.abs(total), keepdims=True))
    scaled = total * scale
    high = eleven_bits(scaled)
    left = eleven_bits(jnp.sum(jnp.where(eye, scaled - high, 0.0), axis=0, keepdims=True))
    out[...] = pack(high, with_factors(tail_of(left), 7, factors))


def square_kernel(own, cols, out, whole):
    at = position()
    left = jnp.zeros((8, LANES), f32)
    for t in range(TPS):
        tail = cols[t, 40:]
        inverse = products(tail)[7:8, FREE : FREE + 1]
        left += tail * inverse
        packed = cols[t] * inverse
        store_rows(whole, MAIN * t, packed)
        store_rows(whole, MAIN * t + 48, low_rows(packed))
        if t % 4 == 0:
            last = last_rows(packed)
        else:
            last = jnp.where(rows_of(8) < PAIR * (t % 4), last, pltpu.roll(last_rows(packed), PAIR * (t % 4), 0))
        if t % 4 == 3:
            store_rows(whole, LAST + 2 * (t - 3), last)
    for block in range(BLOCKS):
        whole[block * LANES + COLS : (block + 1) * LANES, :] = jnp.zeros((LANES - COLS, LANES), f32)
    mine = pl.ds(pl.multiple_of(at[3], LANES), LANES)
    value = whole[mine, :] + jnp.where(own_square(), row_in(left), 0.0)
    whole[mine, :] = value
    trace = jnp.sum(jnp.where(own_square(), value, 0.0), keepdims=True)
    square = jnp.zeros((LANES, LANES), f32)
    for block in range(BLOCKS):
        value = whole[block * LANES : (block + 1) * LANES, :]
        square += value * value
    square = jnp.sum(jnp.where(lanes_of(LANES) < COLS, square, 0.0), keepdims=True)
    out[:40] = own[:40]
    tail = own[40:]
    for i, number in enumerate((square, trace)):
        scale, factors = float16_scale(number)
        rest, words = number * scale, []
        for _ in range(3):
            words.append(eleven_bits(rest))
            rest = rest - words[-1]
        tail = with_row(with_factors(tail, 3 + 2 * i, factors), 4 + 2 * i, FREE, words)
    out[40:] = tail


def first_kernel(rows, whole, out, poly_rows, current_rows, spectral_out, right):
    at = position()
    inverses = {}
    square, trace = jnp.zeros((1, 1), f32), jnp.zeros((1, 1), f32)
    for b, _, packed in each_row_block(rows):
        tail = packed[40:]
        factor = products(tail)[:, FREE : FREE + 1]
        word = (tail[:, FREE + 2 : FREE + 3] + tail[:, FREE + 1 : FREE + 2]) + tail[:, FREE : FREE + 1]
        inverses[b] = factor[7:8]
        square += word[4:5] * factor[3:4]
        trace += word[6:7] * factor[5:6]
    spectral = 2.0 * square / (trace + EPS)
    inverse = 1.0 / spectral
    spectral_out[...] = jnp.broadcast_to(spectral, spectral_out.shape)
    for block in range(BLOCKS):
        part = pl.ds(block * LANES, LANES)
        right[part, :] = (-0.5 * (whole[part, :] * inverse)).astype(bf16)
    mine = pl.ds(pl.multiple_of(at[3], LANES), LANES)
    right[mine, :] = poly(own_square(), whole[mine, :] * inverse).astype(bf16)
    for b, lanes, packed in each_row_block(rows):
        left = row_in(packed[40:])
        for first, part in parts_of(packed):
            eye = eye_of(at, first, part.shape[0], b * COLS)
            current = (jnp.where(eye, part + left, part) * inverses[b]) * inverse
            poly_rows[first : first + part.shape[0], lanes] = poly(eye, current).astype(bf16)
            current_rows[first : first + part.shape[0], lanes] = current.astype(bf16)
    copies(out, pack(dot(poly_rows[...], right[...])))


def second_kernel(current_rows, cols, out_cols, out_rows, right):
    at = position()
    unpack_columns(cols, right)
    current, eye = dot(current_rows[...], right[...]), own_eye(at)
    value = poly(eye, current)
    copies(out_cols, pack(value))
    diagonal = jnp.sum(jnp.where(eye, current, 0.0), axis=0, keepdims=True)
    copies(out_rows, pack(value, tail_of(diagonal)))


def third_kernel(poly_rows, rows, cols, out, right, kept, rows_kept, first_rows, current_rows):
    at = position()
    unpack_columns(cols, right)
    diagonal = [jnp.zeros((count, LANES), f32) for count in (48, 16, 8)]
    for b, lanes, packed in each_row_block(rows):
        row = row_in(packed[40:].astype(f32))
        for i, (first, part) in enumerate(parts_of(packed)):
            count = part.shape[0]
            eye, part = eye_of(at, first, count, b * COLS), part.astype(f32)
            diagonal[i] += jnp.where(eye, row, 0.0)
            first_rows[first : first + count, lanes] = part.astype(bf16)
            current_rows[first : first + count, lanes] = jnp.where(eye, row, -2.0 * part).astype(bf16)
    own = pl.ds(pl.multiple_of(at[3], LANES), LANES)
    product = dot(poly_rows[...], right[...])
    moved = dot(current_rows[...], right[...])
    moved_low = moved.astype(bf16).astype(f32)
    square = dot(first_rows[...], right[...])
    moved_off = moved - moved_low
    kept[0] = first_rows[:, own].astype(f32)
    kept[1] = current_rows[:, own].astype(f32)
    kept[2] = moved_off
    kept[3] = square.astype(bf16).astype(f32) - square
    kept[4] = jnp.broadcast_to(
        jnp.sum(jnp.concatenate(diagonal, axis=0), axis=1, keepdims=True), (ROWS, LANES)
    )
    tail = tail_of(jnp.sum(jnp.where(own_eye(at), moved_off, 0.0), axis=0, keepdims=True))
    product, moved_low = pack(product).astype(bf16), pack(moved_low, tail).astype(bf16)
    for z in range(DEPTH):
        out[z, :SENT] = product
        out[z, SENT:] = moved_low
    mine = right[own, :].astype(f32)
    total = jnp.zeros((LANES, LANES), f32)
    for block in range(BLOCKS):
        value = right[block * LANES : (block + 1) * LANES, :].astype(f32)
        total += value * value
    total = jnp.sum(total, axis=0, keepdims=True)
    on = rows_of(LANES) == lanes_of(LANES)
    rows_kept[...] = jnp.where(
        rows_of(8) == 0,
        jnp.sum(jnp.where(on, mine, 0.0), axis=0, keepdims=True),
        total.astype(bf16).astype(f32) - total,
    )


def fourth_kernel(rows, right, kept, rows_kept, out, product_rows, moved_rows):
    at = position()
    diagonal = [jnp.zeros((count, LANES), f32) for count in (48, 16, 8)]
    for b, lanes, packed in each_row_block(rows):
        moved = packed[SENT:]
        row = row_in(moved[40:].astype(f32))
        for i, (first, part) in enumerate(parts_of(moved)):
            count = part.shape[0]
            diagonal[i] += jnp.where(eye_of(at, first, count, b * COLS), row, 0.0)
            moved_rows[first : first + count, lanes] = part.astype(bf16)
        for first, part in parts_of(packed[:SENT]):
            product_rows[first : first + part.shape[0], lanes] = part.astype(bf16)
    moved_diagonal = jnp.sum(jnp.concatenate(diagonal, axis=0), axis=1, keepdims=True)
    poly_own, current_own, moved_off, square_off, current_diagonal = (kept[i] for i in range(5))
    poly_diagonal, square_diagonal = rows_kept[0:1], rows_kept[1:2]
    eye = own_eye(at)
    off = jnp.where(
        eye,
        moved_off * poly_own + current_own * square_off,
        moved_diagonal * poly_own
        + moved_off * poly_diagonal
        + current_diagonal * square_off
        + current_own * square_diagonal,
    )
    copies(out, pack(poly(eye, dot(moved_rows[...], right[...]) + off)))


def fifth_kernel(product_rows, cols, out, right):
    unpack_columns(cols, right)
    copies(out, pack(dot(product_rows[...], right[...])))


def last_kernel(cols, whole0, whole1, spectral, out_gate, out_up, product):
    for t in range(TPS):
        packed = cols[t]
        product[MAIN * t : MAIN * t + 48, :] = packed
        product[MAIN * t + 48 : MAIN * (t + 1), :] = low_rows(packed).astype(bf16)
    for group in range(TPS // 4):
        product[LAST + 8 * group : LAST + 8 * (group + 1), :] = last_eight(cols, group).astype(bf16)
    ortho = sum(
        lax.dot_general(
            product[side, :], whole[...], (((0,), (0,)), ((), ())), preferred_element_type=f32
        )
        for side, whole in zip(sides(), (whole0, whole1))
    )
    ortho = ortho[:COLS] * jnp.sqrt(2.0 * FF / spectral[0:1, 0:1])
    width = out_gate.shape[1]
    out_gate[...] = ortho[:, :width]
    out_up[...] = ortho[:, width : 2 * width]


def call(kernel, outs, *args, scratch=()):
    vmem = pl.BlockSpec(memory_space=pltpu.VMEM)
    return pl.pallas_call(
        kernel,
        out_shape=[jax.ShapeDtypeStruct(shape, dtype) for shape, dtype in outs],
        in_specs=[vmem] * len(args),
        out_specs=[vmem] * len(outs),
        scratch_shapes=[pltpu.VMEM(shape, dtype) for shape, dtype in scratch],
        compiler_params=pltpu.CompilerParams(vmem_limit_bytes=24 * 2**20),
        name=kernel.__name__,
    )(*args)


def exchange(stacked, axes):
    return lax.all_to_all(stacked, axes, split_axis=0, concat_axis=0, tiled=True)


def both_cores(by_z):
    return lax.all_gather(by_z, "core")


def local(grad_gate, grad_up, moment_gate, moment_up):
    gate_next = BETA * moment_gate + grad_gate
    up_next = BETA * moment_up + grad_up
    half = gate_next.shape[1]
    low = jnp.concatenate([gate_next.astype(bf16), up_next.astype(bf16)], axis=1)
    low = jnp.pad(low, ((0, 0), (0, 3 * LANES - 2 * half)))
    by_z = lax.all_gather(low, "z")
    here = by_z.reshape(SIDE, -1)
    there = lax.ppermute(here, "core", [(0, 1), (1, 0)])
    whole = (here, there)

    right, left = ((KDIM, LANES), bf16), ((ROWS, KDIM), bf16)
    to_tp, to_z = ((TPS, SENT, LANES), bf16), ((DEPTH, SENT, LANES), bf16)
    packed = ((SENT, LANES), f32)

    own = ((LANES, low.shape[1]), bf16)
    (side,) = call(side_kernel, [((SIDE, LANES), f32)], low, here, scratch=[own])
    (shares,) = call(
        gram_kernel, [(to_tp[0], f32)], low, there, side, scratch=[own, ((D, LANES), f32)]
    )
    shares = exchange(shares.astype(f16), TP).astype(f32)
    (sent,) = call(total_kernel, [packed], shares)
    cols = exchange(jnp.broadcast_to(sent.astype(f16), to_tp[0]), TP).astype(f32)
    sent, gram_cols = call(square_kernel, [packed, (right[0], f32)], sent, cols)
    rows = exchange(jnp.broadcast_to(sent.astype(f16), to_z[0]), "z")
    rows = both_cores(rows).astype(f32)
    sent, poly_rows, current_rows, spectral = call(
        first_kernel, [to_tp, left, left, ((8, LANES), f32)], rows, gram_cols, scratch=[right]
    )
    cols, rows = call(
        second_kernel, [to_tp, to_z], current_rows, exchange(sent, TP), scratch=[right]
    )
    rows = both_cores(exchange(rows, "z"))
    cols = exchange(cols, TP)
    rows, right_poly, kept, rows_kept = call(
        third_kernel,
        [((DEPTH, 2 * SENT, LANES), bf16), right, ((5, ROWS, LANES), f32), ((8, LANES), f32)],
        poly_rows,
        rows,
        cols,
        scratch=[left, left],
    )
    rows = both_cores(exchange(rows, "z"))
    cols, product_rows = call(
        fourth_kernel, [to_tp, left], rows, right_poly, kept, rows_kept, scratch=[left]
    )
    (cols,) = call(fifth_kernel, [to_tp], product_rows, exchange(cols, TP), scratch=[right])
    ortho_gate, ortho_up = call(
        last_kernel,
        [((COLS, half), f32)] * 2,
        exchange(cols, TP),
        *whole,
        spectral,
        scratch=[((D, LANES), bf16)],
    )
    return gate_next, up_next, ortho_gate, ortho_up


def solution(mesh):
    split = Mesh(mesh.devices.reshape(DEPTH, 2, 8, 4), ("z", "core", "y", "x"))
    spec = P(FS, TP)
    return jax.shard_map(
        local, mesh=split, in_specs=(spec,) * 4, out_specs=(spec,) * 4, check_vma=False
    )
```
